256 devices in a mesh: ep: 64 (over z, y, core), tp: 4 (over x).
Axes of the slice: x: 4, y: 4, z: 8, core: 2. Of those that a mesh axis runs over, the one named last changes fastest.
Arguments:
- tokens: bfloat16 [3072, 2048], P('ep'), may hold values from -6 to 6
- out_grad: bfloat16 [3072, 2048], P('ep'), may hold values from -4 to 4
- expert_ids: int32 [3072, 4], P('ep'), may hold values from 0 to 63, all different within a row; in each aligned block of 48 rows (0 to 47, 48 to 95, ...) at most 8 rows name the same one
- router_weight: bfloat16 [2048, 64], replicated, may hold values from -0.125 to 0.125
- w_gate: bfloat16 [64, 2048, 1536], P('ep', None, 'tp'), may hold values from -0.125 to 0.125
- w_up: bfloat16 [64, 2048, 1536], P('ep', None, 'tp'), may hold values from -0.125 to 0.125
- w_down: bfloat16 [64, 1536, 2048], P('ep', 'tp'), may hold values from -0.15625 to 0.15625
Outputs:
- token_grad: bfloat16 [3072, 2048], P('ep', 'tp')
- router_grad: float32 [2048, 64], P('tp', 'ep')
- w_gate_grad: bfloat16 [64, 2048, 1536], P('ep', None, 'tp')
- w_up_grad: bfloat16 [64, 2048, 1536], P('ep', None, 'tp')
- w_down_grad: bfloat16 [64, 1536, 2048], P('ep', 'tp')
The draws below stay inside these ranges and needn't reach their ends.
Inputs may be any that keep to these rules, and one draw needn't show every extreme that they name: `expert_ids`: each row names 4 different experts; among the rows of one device no expert is named more than 8 times, and in some devices' rows one expert is named exactly 8 times.
All inputs are finite; a program needn't handle non-finite values.
Results may differ from the reference program's by a relative error of at most 0.0058.
Values may be sent and summed in bfloat16 or wider, within the bound.
A program may use at most 128 MiB of HBM per device.

```python
import math
import jax
import jax.numpy as jnp
import numpy as np
from jax import lax

D = 2048
FF = 1536
TOPK = 4
TOK_DEV = 48
EXPERTS = 64
TOKENS = 3072
CAP = 8
N_EP = 64


def draw_tokens(key, part):
    base_key = jax.random.fold_in(key, 11)
    pick_key = jax.random.fold_in(key, 12)
    base = jax.random.normal(base_key, (TOKENS, D), jnp.float32)
    strong = jax.random.randint(pick_key, (TOKENS, 1), 0, 16) == 0
    values = jnp.where(strong, 4.0 * base, base)
    return jnp.clip(values, -6.0, 6.0).astype(jnp.bfloat16)


def shard_levels(stream_key, shape, pieces, least, high):
    def one(dim, parts):
        steps = jax.random.uniform(jax.random.fold_in(jax.random.fold_in(stream_key, 6), dim), (parts,), jnp.float32, least / len(pieces), high / len(pieces))
        return jnp.repeat(jnp.exp(steps), shape[dim] // parts).reshape((-1,) + (1,) * (len(shape) - dim - 1))

    factor_of = one(*pieces[0])
    for cut in pieces[1:]:
        factor_of = factor_of * one(*cut)
    return factor_of


def shared_out(stream_key, own, number, rows, amount, top, bound, skew):
    ranking = jax.random.permutation(stream_key, amount)
    heavy_load, ordinary = shares(amount, rows * top, bound, skew, True), shares(amount, rows * top, bound, skew, False)
    places = jnp.arange(amount)

    def named(sizes, rotation):
        used = int((sizes > 0).sum())
        fixed = max(1, used // 4)
        moved = fixed + (places - fixed + rotation * (used - fixed)) % max(1, amount - fixed)
        return jnp.zeros((amount,), jnp.int32).at[ranking[jnp.where(places < fixed, places, moved)]].set(jnp.asarray(sizes, jnp.int32))

    sizes = jnp.where(number % 4 == 0, named(heavy_load, number // 4), named(ordinary, number - number // 4 - 1))
    mixed = jax.random.permutation(jax.random.fold_in(own, 3), amount)
    donor, taker = mixed[0:amount // 2 * 2:2], mixed[1:amount // 2 * 2:2]
    slack = jnp.minimum(sizes[donor] - 1, bound - sizes[taker]) // 2
    slack = jnp.where((donor == ranking[0]) | (taker == ranking[0]) | (sizes[taker] == 0), 0, jnp.maximum(slack, 0))
    moved = jax.random.randint(jax.random.fold_in(own, 4), (amount // 2,), 0, 1 << 20) % (slack + 1)
    sizes = sizes.at[donor].add(-moved).at[taker].add(moved)
    items = jnp.searchsorted(jnp.cumsum(sizes), jnp.arange(rows * top), side="right").astype(jnp.int32)
    table = items.reshape(top, rows).T
    table = table[jax.random.permutation(jax.random.fold_in(own, 1), rows)]
    rotation = jax.random.randint(jax.random.fold_in(own, 2), (rows, 1), 0, top)
    return jnp.take_along_axis(table, (jnp.arange(top)[None, :] + rotation) % top, axis=1)


def shares(number_of, total, reach, lean, full):
    portions = [(1 << 20) // math.isqrt(standing ** lean) + 1 for standing in range(1, number_of + 1)]
    largest = reach if full else min(reach, max(-(-total // number_of), total * portions[0] // sum(portions)))
    least = 1 if total - largest >= number_of - 1 else 0
    given, surplus = [largest] + [least] * (number_of - 1), total - largest - least * (number_of - 1)
    while surplus > 0:
        free = [i for i in range(1, number_of) if given[i] < largest] or [i for i in range(1, number_of) if given[i] < reach]
        mass, budget = sum([portions[i] for i in free]), surplus
        for i in free:
            more = min(reach - given[i], max(1, budget * portions[i] // mass), surplus)
            given[i] = given[i] + more
            surplus = surplus - more
    return np.array(given)


def gaussian(key, shape, deviation, bound, pieces=(), kind=jnp.bfloat16):
    values = deviation * jax.random.normal(key, shape, jnp.float32)
    if pieces:
        values = values * shard_levels(key, shape, pieces, -0.22, 0.18)
    return jnp.clip(values, -bound, bound).astype(kind)


def setup_inputs(seed: int = 0) -> dict:
    seeds = jax.random.split(jax.random.key(seed), 8)
    tokens = draw_tokens(jax.random.fold_in(seeds[7], 71), 0)
    out_grad = gaussian(seeds[1], (TOKENS, D), 0.3, 4.0, ((0, 64),))
    expert_ids_keys = jax.random.split(jax.random.fold_in(seeds[2], 1), TOKENS // TOK_DEV)
    expert_ids_turns = jax.random.permutation(jax.random.fold_in(seeds[2], 3), TOKENS // TOK_DEV)
    expert_ids = jax.vmap(lambda own, number: shared_out(jax.random.fold_in(seeds[2], 2), own, number, TOK_DEV, EXPERTS, TOPK, CAP, 1))(expert_ids_keys, expert_ids_turns).reshape((TOKENS, TOPK))
    router_weight = gaussian(seeds[3], (D, EXPERTS), D ** -0.5, 0.125)
    w_gate = gaussian(seeds[4], (EXPERTS, D, FF), D ** -0.5, 0.125, ((0, 64), (2, 4)))
    w_up = gaussian(seeds[5], (EXPERTS, D, FF), D ** -0.5, 0.125, ((0, 64), (2, 4)))
    w_down = gaussian(seeds[6], (EXPERTS, FF, D), FF ** -0.5, 0.15625, ((0, 64), (1, 4)))
    return {"tokens": tokens, "out_grad": out_grad, "expert_ids": expert_ids, "router_weight": router_weight, "w_gate": w_gate, "w_up": w_up, "w_down": w_down}


def activation_parts(gate_pre, up_pre):
    glu = jnp.minimum(gate_pre, 7.0)
    linear = jnp.clip(up_pre, -7.0, 7.0)
    sigma = jax.nn.sigmoid(1.702 * glu)
    act_value = glu * sigma
    hidden = (linear + 1.0) * act_value
    slope = (linear + 1.0) * (sigma + 1.702 * glu * sigma * (1.0 - sigma))
    slope = jnp.where(gate_pre < 7.0, slope, 0.0)
    up_slope = jnp.where((up_pre > -7.0) & (up_pre < 7.0), act_value, 0.0)
    return hidden, slope, up_slope


def reference(tokens, out_grad, expert_ids, router_weight, w_gate, w_up, w_down):
    logits = jnp.dot(tokens, router_weight, preferred_element_type=jnp.float32)
    chosen = jnp.take_along_axis(logits, expert_ids, axis=1)
    gate_values = jax.nn.softmax(chosen, axis=-1)
    assign_total = TOKENS * TOPK
    slot_total = N_EP * CAP
    flat_ids = expert_ids.reshape(-1)
    flat_tok = (jnp.arange(assign_total, dtype=jnp.int32) // TOPK).astype(jnp.int32)
    flat_gate = gate_values.reshape(-1)

    def per_expert(carry, inputs):
        token_acc, score_acc = carry
        gate_mat, up_mat, down_mat, expert = inputs
        picked = jnp.nonzero(flat_ids == expert, size=slot_total, fill_value=assign_total)[0].astype(jnp.int32)
        valid = picked < assign_total
        safe_pick = jnp.minimum(picked, assign_total - 1).astype(jnp.int32)
        tok_rows = flat_tok[safe_pick]
        inputs_rows = tokens[tok_rows]
        grad_rows = out_grad[tok_rows]
        weight_rows = jnp.where(valid, flat_gate[safe_pick], 0.0)
        gate_pre = jnp.dot(inputs_rows, gate_mat, preferred_element_type=jnp.float32)
        up_pre = jnp.dot(inputs_rows, up_mat, preferred_element_type=jnp.float32)
        hidden, slope, up_slope = activation_parts(gate_pre, up_pre)
        back_proj = jnp.dot(grad_rows, down_mat.T, preferred_element_type=jnp.float32)
        gate_score = jnp.sum(hidden * back_proj, axis=1)
        d_hidden = weight_rows[:, None] * back_proj
        d_gate_pre = (d_hidden * slope).astype(jnp.bfloat16)
        d_up_pre = (d_hidden * up_slope).astype(jnp.bfloat16)
        weighted = (weight_rows[:, None] * hidden).astype(jnp.bfloat16)
        down_grad = jnp.dot(weighted.T, grad_rows, preferred_element_type=jnp.float32).astype(jnp.bfloat16)
        gate_grad = jnp.dot(inputs_rows.T, d_gate_pre, preferred_element_type=jnp.float32).astype(jnp.bfloat16)
        up_grad = jnp.dot(inputs_rows.T, d_up_pre, preferred_element_type=jnp.float32).astype(jnp.bfloat16)
        token_part = jnp.dot(d_gate_pre, gate_mat.T, preferred_element_type=jnp.float32)
        token_part = token_part + jnp.dot(d_up_pre, up_mat.T, preferred_element_type=jnp.float32)
        token_acc = token_acc.at[tok_rows].add(jnp.where(valid[:, None], token_part, 0.0))
        score_acc = score_acc.at[safe_pick].add(jnp.where(valid, gate_score, 0.0))
        return (token_acc, score_acc), (gate_grad, up_grad, down_grad)

    start_carry = (jnp.zeros((TOKENS, D), jnp.float32), jnp.zeros((assign_total,), jnp.float32))
    expert_list = jnp.arange(EXPERTS, dtype=jnp.int32)
    (token_acc, score_acc), (w_gate_grad, w_up_grad, w_down_grad) = lax.scan(
        per_expert, start_carry, (w_gate, w_up, w_down, expert_list))
    gate_score = score_acc.reshape(TOKENS, TOPK)
    d_chosen = gate_values * (gate_score - jnp.sum(gate_values * gate_score, axis=-1, keepdims=True))
    one_hot = (expert_ids[:, :, None] == jnp.arange(EXPERTS, dtype=jnp.int32)[None, None, :]).astype(jnp.float32)
    d_logits = jnp.sum(d_chosen[:, :, None] * one_hot, axis=1)
    router_grad = jnp.dot(tokens.astype(jnp.float32).T, d_logits, precision=lax.Precision.HIGHEST)
    router_part = jnp.dot(d_logits, router_weight.astype(jnp.float32).T, precision=lax.Precision.HIGHEST)
    token_grad = (token_acc + router_part).astype(jnp.bfloat16)
    return token_grad, router_grad, w_gate_grad, w_up_grad, w_down_grad
```

```python
import functools

import jax
import jax.numpy as jnp
from jax import lax
from jax.experimental import pallas as pl
from jax.experimental.pallas import tpu as pltpu
from jax.sharding import PartitionSpec as P

MESH = pl.DeviceIdType.MESH
F32 = jnp.float32
BF16 = jnp.bfloat16
NK = 8
NE = 8
CAP = 8
PAIR_OF = (0, 2, 1, 4, 3, 6, 5, 7)


def dot_last(a, b):
    return lax.dot_general(a, b, (((1,), (1,)), ((), ())), preferred_element_type=F32)


def dot_first(a, b):
    return lax.dot_general(a, b, (((0,), (0,)), ((), ())), preferred_element_type=F32)


def dot(a, b):
    return jnp.dot(a, b, preferred_element_type=F32)


def step_kernel(
    tok_hbm,
    grad_hbm,
    ids_ref,
    rw_ref,
    wg_hbm,
    wu_hbm,
    wd_hbm,
    tg_ref,
    rg_ref,
    gg_hbm,
    ug_hbm,
    dg_hbm,
    tokv,
    wg,
    wu,
    wd,
    zbuf,
    square,
    info,
    infoz,
    infoe,
    einfo,
    pbuf,
    ysend,
    buf,
    dgu,
    wtd,
    dxq,
    r1,
    acc,
    s2,
    r2,
    yret,
    yrr,
    wsend,
    wrecv,
    sx,
    sy,
    syr,
    szs,
    smat,
    dmat,
    dz,
    dys,
    de,
    stage,
    stage2,
    ld,
    zss,
    zrs,
    iss,
    irs,
    ess,
    ers,
    yss,
    yrs,
    xss,
    xrs,
    r1s,
    r1r,
    r2s,
    r2r,
    xcs,
    xcr,
    sys_,
    syr_,
    szs_,
    szr_,
    vss,
    vrs,
    wss,
    wrs,
    dzs_,
    dzr_,
    dys_,
    dyr_,
    outs,
):
    ep = lax.axis_index("ep")
    x = lax.axis_index("tp")
    z = ep // NE
    yc = ep % NE
    par = x % 2
    odd = x % 2
    near_a = x + 1 - 2 * odd
    near_b = (x + 3 + 2 * odd) % 4
    far = (x + 2) % 4
    right = (x + 1) % 4
    left = (x + 3) % 4

    def remote(src, dst, ss, rs, e, t):
        return pltpu.make_async_remote_copy(
            src_ref=src,
            dst_ref=dst,
            send_sem=ss,
            recv_sem=rs,
            device_id={"ep": e, "tp": t},
            device_id_type=MESH,
        )

    def z_of(k):
        h = (k + 1) // 2
        s = 1 - 2 * ((k + 1) % 2)
        return (z + s * h + NK) % NK

    def at_z(zz):
        return zz * NE + yc

    def at_e(j):
        return z * NE + j

    barrier = pltpu.get_barrier_semaphore()
    for d in range(1, NK):
        pl.semaphore_signal(
            barrier, inc=1, device_id={"ep": at_z((z + d) % NK), "tp": x}, device_id_type=MESH
        )
    for d in range(1, NE):
        pl.semaphore_signal(
            barrier, inc=1, device_id={"ep": at_e((yc + d) % NE), "tp": x}, device_id_type=MESH
        )
    for d in range(1, 4):
        pl.semaphore_signal(
            barrier, inc=1, device_id={"ep": ep, "tp": (x + d) % 4}, device_id_type=MESH
        )

    load_tok = pltpu.make_async_copy(tok_hbm, tokv, ld.at[0])
    load_tok.start()

    @pl.when(par == 0)
    def _():
        pltpu.make_async_copy(tok_hbm, zbuf.at[0], ld.at[1]).start()

    @pl.when(par == 1)
    def _():
        pltpu.make_async_copy(grad_hbm, zbuf.at[0], ld.at[1]).start()

    load_g = pltpu.make_async_copy(wg_hbm, wg, ld.at[2])
    load_u = pltpu.make_async_copy(wu_hbm, wu, ld.at[3])
    load_d = pltpu.make_async_copy(wd_hbm, wd, ld.at[4])
    load_g.start()
    load_u.start()
    load_d.start()

    load_tok.wait()
    n_tok = tokv.shape[0]
    n_exp = rw_ref.shape[1]
    logits = dot(tokv[...], rw_ref[...])
    lane_e = lax.broadcasted_iota(jnp.int32, (n_tok, n_exp), 1)
    hit = jnp.zeros((n_tok, n_exp), F32)
    for k in range(ids_ref.shape[1]):
        hit = hit + jnp.where(ids_ref[:, k : k + 1] == lane_e, 1.0, 0.0)
    chosen = hit > 0.0
    top = jnp.max(jnp.where(chosen, logits, -jnp.inf), axis=1, keepdims=True)
    expd = jnp.where(chosen, jnp.exp(jnp.where(chosen, logits - top, 0.0)), 0.0)
    gates = expd / jnp.sum(expd, axis=1, keepdims=True)
    row = lax.broadcasted_iota(jnp.int32, (n_tok, n_tok), 0)
    col = lax.broadcasted_iota(jnp.int32, (n_tok, n_tok), 1)
    earlier = jnp.where(col < row, 1.0, 0.0).astype(BF16)
    rank = dot(earlier, hit.astype(BF16))
    square[...] = jnp.full(square.shape, -1.0, F32)
    square[0:n_tok, 0:n_exp] = jnp.where(chosen, rank, -1.0)
    info[0] = square[...].T[0:n_exp, :]
    square[...] = jnp.zeros(square.shape, F32)
    square[0:n_tok, 0:n_exp] = gates
    info[1] = square[...].T[0:n_exp, :]

    pl.semaphore_wait(barrier, (NK - 1) + (NE - 1) + 3)

    pltpu.make_async_copy(tok_hbm, zbuf.at[0], ld.at[1]).wait()

    def z_copy(k, part=None):
        if part is None:
            src, dst, rs = zbuf.at[k], zbuf.at[k + 2], zrs.at[k + 2]
        else:
            half = zbuf.shape[2] // 2
            cols = pl.ds(part * half, half)
            src, dst, rs = zbuf.at[k, :, cols], zbuf.at[7, :, cols], zrs.at[8 - part]
        s = 1 - 2 * ((k + 1) % 2)
        return remote(src, dst, zss.at[k], rs, at_z((z - s + NK) % NK), x)

    z_left = remote(zbuf.at[0], zbuf.at[1], zss.at[0], zrs.at[1], at_z((z + NK - 1) % NK), x)
    z_right = remote(zbuf.at[0], zbuf.at[2], zss.at[7], zrs.at[2], at_z((z + 1) % NK), x)
    z_left.start()
    z_right.start()

    def info_copy(k):
        zz = z_of(k)
        return remote(
            info.at[:, pl.ds(pl.multiple_of(zz * NE, NE), NE)],
            infoz.at[PAIR_OF[k]],
            iss.at[k],
            irs.at[PAIR_OF[k]],
            at_z(zz),
            x,
        )

    for k in range(1, NK):
        info_copy(k).start()
    own = pl.ds(pl.multiple_of(z * NE, NE), NE)
    infoz[0, 0] = info[0, own, :]
    infoz[0, 1] = info[1, own, :]

    def info_wait(k):
        remote(infoz.at[k], infoz.at[k], iss.at[k], irs.at[k], ep, x).wait_recv()

    def y_copy(k, d):
        j = (yc + d) % NE
        return remote(
            ysend.at[k, j], buf.at[par, k * NE + yc], yss.at[k, d], yrs.at[k, d], at_e(j), x
        )

    def y_wait(k, d):
        j = (yc + NE - d) % NE
        remote(
            ysend.at[k, 0], buf.at[par, k * NE + j], yss.at[k, d], yrs.at[k, d], ep, x
        ).wait_recv()

    def z_wait(k):
        @pl.when((k >= 1) & (k <= 6))
        def _():
            remote(zbuf.at[k], zbuf.at[k], zss.at[0], zrs.at[k], ep, x).wait_recv()

        @pl.when(k == 7)
        def _():
            half = zbuf.shape[2] // 2
            for part in range(2):
                cols = pl.ds(part * half, half)
                remote(
                    zbuf.at[7, :, cols], zbuf.at[7, :, cols], zss.at[0], zrs.at[8 - part], ep, x
                ).wait_recv()

    def select_block(k):
        z_wait(k)

        @pl.when((k >= 1) & (k <= 4))
        def _():
            z_copy(k).start()

        @pl.when(k == 5)
        def _():
            z_copy(5, 1).start()

        @pl.when(k == 6)
        def _():
            z_copy(6, 0).start()

        code = infoz[k, 0]
        want = lax.broadcasted_iota(jnp.int32, (NE, CAP, 128), 1).astype(F32)
        place = (jnp.broadcast_to(code[:, None, :], (NE, CAP, 128)) == want).astype(F32)
        place = place.reshape(NE * CAP, 128).astype(BF16)
        pbuf[k] = place
        block = zbuf[k]
        for q in range(4):
            cols = slice(512 * q, 512 * (q + 1))
            rows = dot(place[:, 0:n_tok], block[:, cols])
            ysend[k, :, :, cols] = rows.astype(BF16).reshape(NE, CAP, 512)
        buf[par, k * NE + yc] = ysend[k, yc]
        for d in (1, 7, 2, 6, 3, 5, 4):
            y_copy(k, d).start()

    half_e = NE // 2

    def x_copy(k, side):
        rows = pl.ds(k * NE + side * half_e, half_e)
        return remote(
            buf.at[par, rows],
            buf.at[par, rows],
            xss.at[k, side],
            xrs.at[k, side],
            ep,
            left if side else right,
        )

    def x_wait(k, side):
        rows = pl.ds(k * NE + side * half_e, half_e)
        remote(
            buf.at[1 - par, rows], buf.at[1 - par, rows], xss.at[k, side], xrs.at[k, side], ep, x
        ).wait_recv()

    def pass_on(k):
        for d in range(1, NE):
            y_wait(k, d)
        x_copy(k, 0).start()
        x_copy(k, 1).start()

    def einfo_copy(d):
        j = (yc + d) % NE
        return remote(infoe.at[j], einfo.at[yc], ess.at[d], ers.at[d], at_e(j), x)

    def einfo_wait(d):
        j = (yc + NE - d) % NE
        remote(infoe.at[0], einfo.at[j], ess.at[d], ers.at[d], ep, x).wait_recv()

    def spread_info():
        for e in range(NE):
            for part in range(2):
                infoe[e, part] = jnp.concatenate(
                    [infoz[k, part, e : e + 1, :] for k in range(NK)], axis=0
                )
        einfo[yc] = infoe[yc]
        for d in range(1, NE):
            einfo_copy(d).start()

    def slot_rows(part, k):
        return jnp.concatenate([einfo[j, part, pl.ds(k, 1), :] for j in range(NE)], axis=0)

    def score_copy(m, d):
        t = (x + d) % 4
        rows = pl.ds(m * 16, 16)
        return remote(sx.at[0, rows], sx.at[4 - d, rows], xcs.at[m, d], xcr.at[m, d], ep, t)

    def score_wait(m, d):
        rows = pl.ds(m * 16, 16)
        remote(sx.at[0, rows], sx.at[4 - d, rows], xcs.at[m, d], xcr.at[m, d], ep, x).wait_recv()

    def halves_copy(m, which, slot):
        k = 2 * m + which
        peer = near_b if which else near_a
        q = far if slot else peer
        rows = pl.ds(k * NE, NE)
        return remote(
            dxq.at[q, rows], r1.at[slot, rows], r1s.at[k, slot], r1r.at[k, slot], ep, peer
        )

    def halves_wait(m, which, slot):
        k = 2 * m + which
        rows = pl.ds(k * NE, NE)
        remote(
            r1.at[slot, rows], r1.at[slot, rows], r1s.at[k, slot], r1r.at[k, slot], ep, x
        ).wait_recv()

    def compute(m):
        for k in (2 * m, 2 * m + 1):
            x_wait(k, 0)
            x_wait(k, 1)
        rows = pl.ds(m * 16, 16)
        flat = pl.ds(pl.multiple_of(m * 128, 128), 128)
        xin = buf[0, rows].reshape(128, 2048)
        gin = buf[1, rows].reshape(128, 2048)
        gate_pre = dot(xin, wg[...])
        up_pre = dot(xin, wu[...])
        back = dot_last(gin, wd[...])
        code = jnp.concatenate([slot_rows(0, 2 * m), slot_rows(0, 2 * m + 1)], axis=0)
        gate = jnp.concatenate([slot_rows(1, 2 * m), slot_rows(1, 2 * m + 1)], axis=0)
        want = lax.broadcasted_iota(jnp.int32, (16, CAP, 128), 1).astype(F32)
        mine = jnp.broadcast_to(code[:, None, :], (16, CAP, 128)) == want
        wide = jnp.where(mine, jnp.broadcast_to(gate[:, None, :], (16, CAP, 128)), 0.0)
        weight = jnp.sum(wide.reshape(128, 128), axis=1, keepdims=True)
        glu = jnp.minimum(gate_pre, 7.0)
        lin1 = jnp.clip(up_pre, -7.0, 7.0) + 1.0
        sig = jax.nn.sigmoid(1.702 * glu)
        act = glu * sig
        hidden = lin1 * act
        slope = lin1 * (sig + 1.702 * glu * sig * (1.0 - sig))
        slope = jnp.where(gate_pre < 7.0, slope, 0.0)
        up_slope = jnp.where((up_pre > -7.0) & (up_pre < 7.0), act, 0.0)
        score = jnp.sum(hidden * back, axis=1, keepdims=True)
        d_hidden = weight * back
        d_gate = (d_hidden * slope).astype(BF16)
        d_up = (d_hidden * up_slope).astype(BF16)
        dgu[flat, 0:384] = d_gate
        dgu[flat, 384:768] = d_up
        wtd[flat, :] = (weight * hidden).astype(BF16)
        lane = lax.broadcasted_iota(jnp.int32, (16, CAP, 128), 2)
        sub = lax.broadcasted_iota(jnp.int32, (16, CAP, 128), 1)
        spread = jnp.broadcast_to(score, (128, 128)).reshape(16, CAP, 128)
        sx[0, rows] = jnp.sum(jnp.where(lane == sub, spread, 0.0), axis=1)
        for d in range(1, 4):
            score_copy(m, d).start()
        for q in range(4):
            cols = slice(512 * q, 512 * (q + 1))
            part = dot_last(d_gate, wg[cols, :]) + dot_last(d_up, wu[cols, :])
            dxq[q, rows] = part.astype(BF16).reshape(16, CAP, 512)
        for slot in (1, 0):
            for which in range(2):
                halves_copy(m, which, slot).start()

    def quarter_copy(m, which):
        k = 2 * m + which
        rows = pl.ds(k * NE, NE)
        return remote(
            s2.at[rows], r2.at[rows], r2s.at[k], r2r.at[k], ep, near_a if which else near_b
        )

    def reduce_first(m):
        for which in range(2):
            k = 2 * m + which
            rows = pl.ds(k * NE, NE)
            halves_wait(m, which, 1)
            s2[rows] = (
                dxq[near_a if which else near_b, rows].astype(F32) + r1[1, rows].astype(F32)
            ).astype(BF16)
            quarter_copy(m, which).start()
        for which in range(2):
            k = 2 * m + which
            rows = pl.ds(k * NE, NE)
            halves_wait(m, which, 0)
            acc[rows] = dxq[x, rows].astype(F32) + r1[0, rows].astype(F32)

    def back_copy(m, d):
        j = (yc + d) % NE
        ks = pl.ds(2 * m, 2)
        return remote(yret.at[j, ks], yrr.at[yc, ks], vss.at[m, d], vrs.at[m, d], at_e(j), x)

    def back_wait(m, d):
        j = (yc + NE - d) % NE
        ks = pl.ds(2 * m, 2)
        remote(yret.at[0, ks], yrr.at[j, ks], vss.at[m, d], vrs.at[m, d], ep, x).wait_recv()

    def reduce_second(m):
        for which in range(2):
            k = 2 * m + which
            rows = pl.ds(k * NE, NE)
            remote(s2.at[rows], r2.at[rows], r2s.at[k], r2r.at[k], ep, x).wait_recv()
            total = (acc[rows] + r2[rows].astype(F32)).astype(BF16)
            for j in range(NE):
                yret[j, k] = total[j]
        yrr[yc, pl.ds(2 * m, 2)] = yret[yc, pl.ds(2 * m, 2)]
        for d in (1, 7, 2, 6, 3, 5, 4):
            back_copy(m, d).start()

    def home_copy(k):
        return remote(
            wsend.at[k], wrecv.at[PAIR_OF[k]], wss.at[k], wrs.at[PAIR_OF[k]], at_z(z_of(k)), x
        )

    def combine(m):
        for d in range(1, NE):
            back_wait(m, d)
        for which in range(2):
            k = 2 * m + which
            rows = jnp.concatenate([yrr[j, k] for j in range(NE)], axis=0)
            wsend[k] = dot_first(pbuf[k][:, 0:n_tok], rows).astype(BF16)
            if k > 0:
                home_copy(k).start()

    for k in range(1, NK):
        info_wait(k)
    spread_info()

    def round_of(it, carry):
        @pl.when(it < NK)
        def _():
            select_block(it)

        @pl.when((it >= 1) & (it <= NK))
        def _():
            pass_on(it - 1)

        @pl.when(it == 3)
        def _():
            load_g.wait()
            load_u.wait()
            load_d.wait()
            for d in range(1, NE):
                einfo_wait(d)

        @pl.when((it >= 3) & (it % 2 == 1))
        def _():
            compute((it - 3) // 2)

        return carry

    lax.fori_loop(0, 10, round_of, 0)

    for m in range(4):
        for d in range(1, 4):
            score_wait(m, d)
    sx[1] = (sx[0] + sx[1]) + (sx[2] + sx[3])

    def sy_copy(d):
        j = (yc + d) % NE
        return remote(sy.at[j], syr.at[yc], sys_.at[d], syr_.at[d], at_e(j), x)

    for j in range(NE):
        sy[j] = jnp.concatenate([sx[1, k * NE + j : k * NE + j + 1, :] for k in range(NK)], axis=0)
    syr[yc] = sy[yc]
    for d in range(1, NE):
        sy_copy(d).start()

    reduce_first(0)
    reduce_first(1)

    def out_copy(i, slot):
        rows = pl.ds(pl.multiple_of(i * 256, 256), 256)
        return (
            pltpu.make_async_copy(
                stage.at[slot, :, pl.ds(0, 384)], gg_hbm.at[rows], outs.at[0, slot]
            ),
            pltpu.make_async_copy(
                stage.at[slot, :, pl.ds(384, 384)], ug_hbm.at[rows], outs.at[1, slot]
            ),
            pltpu.make_async_copy(stage2.at[slot], dg_hbm.at[:, rows], outs.at[2, slot]),
        )

    def weight_tile(i, carry):
        cols = pl.ds(pl.multiple_of(i * 256, 256), 256)
        xs = buf[0, :, :, cols].reshape(512, 256)
        stage[i] = dot_first(xs, dgu[...]).astype(BF16)
        gs = buf[1, :, :, cols].reshape(512, 256)
        stage2[i] = dot_first(wtd[...], gs).astype(BF16)
        for c in out_copy(i, i):
            c.start()
        return carry

    lax.fori_loop(0, 2, weight_tile, 0)

    def sz_copy(k):
        zz = z_of(k)
        return remote(
            szs.at[k],
            smat.at[pl.ds(pl.multiple_of(z * NE, NE), NE)],
            szs_.at[k],
            szr_.at[PAIR_OF[k]],
            at_z(zz),
            x,
        )

    for d in range(1, NE):
        j = (yc + NE - d) % NE
        remote(sy.at[0], syr.at[j], sys_.at[d], syr_.at[d], ep, x).wait_recv()
    for k in range(NK):
        szs[k] = jnp.concatenate([syr[e, k : k + 1, :] for e in range(NE)], axis=0)
    for k in range(1, NK):
        sz_copy(k).start()
    smat[own, :] = szs[0]

    reduce_first(2)
    reduce_first(3)
    reduce_second(0)
    reduce_second(1)
    reduce_second(2)
    reduce_second(3)

    lax.fori_loop(2, 5, weight_tile, 0)

    for k in range(1, NK):
        zz = z_of(k)
        rows = pl.ds(pl.multiple_of(zz * NE, NE), NE)
        remote(szs.at[k], smat.at[rows], szs_.at[k], szr_.at[k], ep, x).wait_recv()
    score_at = jnp.zeros((n_exp, 128), F32)
    for r in range(CAP):
        score_at = score_at + jnp.where(info[0] == float(r), smat[:, r : r + 1], 0.0)
    gate_t = info[1]
    mean = jnp.sum(gate_t * score_at, axis=0, keepdims=True)
    dmat[...] = jnp.where(info[0] >= 0.0, gate_t * (score_at - mean), 0.0)

    def dz_copy(k):
        zz = z_of(k)
        return remote(
            dmat.at[pl.ds(pl.multiple_of(zz * NE, NE), NE)],
            dz.at[PAIR_OF[k]],
            dzs_.at[k],
            dzr_.at[PAIR_OF[k]],
            at_z(zz),
            x,
        )

    for k in range(1, NK):
        dz_copy(k).start()
    dz[0] = dmat[own, :]

    for m in range(4):
        combine(m)

    lax.fori_loop(5, 8, weight_tile, 0)

    def dy_copy(d):
        j = (yc + d) % NE
        return remote(dys.at[j], de.at[yc], dys_.at[d], dyr_.at[d], at_e(j), x)

    for k in range(1, NK):
        remote(dz.at[k], dz.at[k], dzs_.at[k], dzr_.at[k], ep, x).wait_recv()
    for e in range(NE):
        dys[e] = jnp.concatenate([dz[k, e : e + 1, :] for k in range(NK)], axis=0)
    for d in range(1, NE):
        dy_copy(d).start()
    de[yc] = dys[yc]

    d_t = dmat[...]
    d_hi = d_t.astype(BF16)
    d_lo = (d_t - d_hi.astype(F32)).astype(BF16)
    x_rows = pl.ds(pl.multiple_of(x * 512, 512), 512)
    rw_x = rw_ref[x_rows, :]

    def across(d):
        return lax.dot_general(d, rw_x, (((0,), (1,)), ((), ())), preferred_element_type=F32)

    total = (across(d_hi) + across(d_lo))[0:n_tok, :] + wsend[0].astype(F32)
    for k in range(1, NK):
        remote(wsend.at[k], wrecv.at[k], wss.at[k], wrs.at[k], ep, x).wait_recv()
        total = total + wrecv[k].astype(F32)
    tg_ref[...] = total.astype(BF16)

    for d in range(1, NE):
        j = (yc + NE - d) % NE
        remote(dys.at[0], de.at[j], dys_.at[d], dyr_.at[d], ep, x).wait_recv()
    want = lax.broadcasted_iota(jnp.int32, (NE, CAP, 128), 1).astype(F32)
    sums = jnp.zeros((CAP, 512), F32)
    for k in range(NK):
        code = slot_rows(0, k)
        d_rows = jnp.concatenate([de[j, k : k + 1, :] for j in range(NE)], axis=0)
        mine = jnp.broadcast_to(code[:, None, :], (NE, CAP, 128)) == want
        wide = jnp.where(mine, jnp.broadcast_to(d_rows[:, None, :], (NE, CAP, 128)), 0.0)
        slot_d = jnp.sum(wide, axis=2, keepdims=True)
        rows = buf[0, k * NE : (k + 1) * NE, :, x_rows].astype(F32)
        sums = sums + jnp.sum(slot_d * rows, axis=0)
    rg_ref[...] = jnp.sum(sums, axis=0, keepdims=True)

    z_left.wait_send()
    z_right.wait_send()
    for k in (1, 2, 3, 4):
        z_copy(k).wait_send()
    z_copy(5, 1).wait_send()
    z_copy(6, 0).wait_send()
    for k in range(1, NK):
        info_copy(k).wait_send()
        home_copy(k).wait_send()
        sz_copy(k).wait_send()
        dz_copy(k).wait_send()
    for d in range(1, NE):
        einfo_copy(d).wait_send()
        sy_copy(d).wait_send()
        dy_copy(d).wait_send()

    def drain(k, carry):
        for d in range(1, NE):
            y_copy(k, d).wait_send()
        x_copy(k, 0).wait_send()
        x_copy(k, 1).wait_send()
        for c in out_copy(k, k):
            c.wait()
        return carry

    lax.fori_loop(0, NK, drain, 0)
    for m in range(4):
        for d in range(1, 4):
            score_copy(m, d).wait_send()
        for d in range(1, NE):
            back_copy(m, d).wait_send()
        for which in range(2):
            halves_copy(m, which, 0).wait_send()
            halves_copy(m, which, 1).wait_send()
            quarter_copy(m, which).wait_send()


def per_device(tokens, out_grad, expert_ids, router_weight, w_gate, w_up, w_down):
    n_tok, width = tokens.shape
    n_exp = router_weight.shape[1]
    ff = w_gate.shape[2]
    quarter = width // 4
    any_space = pl.BlockSpec(memory_space=pl.ANY)
    vmem = pl.BlockSpec(memory_space=pltpu.VMEM)
    dma = pltpu.SemaphoreType.DMA
    slots = NK * NE
    scratch = [
        pltpu.VMEM((n_tok, width), BF16),
        pltpu.VMEM((width, ff), BF16),
        pltpu.VMEM((width, ff), BF16),
        pltpu.VMEM((ff, width), BF16),
        pltpu.VMEM((NK, n_tok, width), BF16),
        pltpu.VMEM((128, 128), F32),
        pltpu.VMEM((2, n_exp, 128), F32),
        pltpu.VMEM((NK, 2, NE, 128), F32),
        pltpu.VMEM((NE, 2, NK, 128), F32),
        pltpu.VMEM((NE, 2, NK, 128), F32),
        pltpu.VMEM((NK, NE * CAP, 128), BF16),
        pltpu.VMEM((NK, NE, CAP, width), BF16),
        pltpu.VMEM((2, slots, CAP, width), BF16),
        pltpu.VMEM((slots * CAP, 2 * ff), BF16),
        pltpu.VMEM((slots * CAP, ff), BF16),
        pltpu.VMEM((4, slots, CAP, quarter), BF16),
        pltpu.VMEM((2, slots, CAP, quarter), BF16),
        pltpu.VMEM((slots, CAP, quarter), F32),
        pltpu.VMEM((slots, CAP, quarter), BF16),
        pltpu.VMEM((slots, CAP, quarter), BF16),
        pltpu.VMEM((NE, NK, CAP, quarter), BF16),
        pltpu.VMEM((NE, NK, CAP, quarter), BF16),
        pltpu.VMEM((NK, n_tok, quarter), BF16),
        pltpu.VMEM((NK, n_tok, quarter), BF16),
        pltpu.VMEM((4, slots, 128), F32),
        pltpu.VMEM((NE, NK, 128), F32),
        pltpu.VMEM((NE, NK, 128), F32),
        pltpu.VMEM((NK, NE, 128), F32),
        pltpu.VMEM((n_exp, 128), F32),
        pltpu.VMEM((n_exp, 128), F32),
        pltpu.VMEM((NK, NE, 128), F32),
        pltpu.VMEM((NE, NK, 128), F32),
        pltpu.VMEM((NE, NK, 128), F32),
        pltpu.VMEM((8, 256, 2 * ff), BF16),
        pltpu.VMEM((8, ff, 256), BF16),
        dma((8,)),
        dma((8,)),
        dma((9,)),
        dma((8,)),
        dma((8,)),
        dma((8,)),
        dma((8,)),
        dma((8, 8)),
        dma((8, 8)),
        dma((8, 2)),
        dma((8, 2)),
        dma((8, 2)),
        dma((8, 2)),
        dma((8,)),
        dma((8,)),
        dma((4, 4)),
        dma((4, 4)),
        dma((8,)),
        dma((8,)),
        dma((8,)),
        dma((8,)),
        dma((4, 8)),
        dma((4, 8)),
        dma((8,)),
        dma((8,)),
        dma((8,)),
        dma((8,)),
        dma((8,)),
        dma((8,)),
        dma((3, 8)),
    ]
    out = pl.pallas_call(
        step_kernel,
        name="moe_backward",
        out_shape=(
            jax.ShapeDtypeStruct((n_tok, quarter), BF16),
            jax.ShapeDtypeStruct((1, quarter), F32),
            jax.ShapeDtypeStruct((width, ff), BF16),
            jax.ShapeDtypeStruct((width, ff), BF16),
            jax.ShapeDtypeStruct((ff, width), BF16),
        ),
        in_specs=[any_space, any_space, vmem, vmem, any_space, any_space, any_space],
        out_specs=(vmem, vmem, any_space, any_space, any_space),
        scratch_shapes=scratch,
        compiler_params=pltpu.CompilerParams(
            collective_id=0, has_side_effects=True, vmem_limit_bytes=56 * 1024 * 1024
        ),
    )(tokens, out_grad, expert_ids, router_weight, w_gate[0], w_up[0], w_down[0])
    token_grad, router_grad, gate_grad, up_grad, down_grad = out
    return (
        token_grad,
        router_grad.reshape(quarter, 1),
        gate_grad[None],
        up_grad[None],
        down_grad[None],
    )


def solution(mesh):
    in_specs = (
        P("ep", None),
        P("ep", None),
        P("ep", None),
        P(),
        P("ep", None, "tp"),
        P("ep", None, "tp"),
        P("ep", "tp", None),
    )
    out_specs = (
        P("ep", "tp"),
        P("tp", "ep"),
        P("ep", None, "tp"),
        P("ep", None, "tp"),
        P("ep", "tp", None),
    )
    return jax.shard_map(
        per_device, mesh=mesh, in_specs=in_specs, out_specs=out_specs, check_vma=False
    )
```

```python
import functools

import jax
import jax.numpy as jnp
from jax import lax
from jax.experimental import pallas as pl
from jax.experimental.pallas import tpu as pltpu
from jax.sharding import PartitionSpec as P

MESH = pl.DeviceIdType.MESH
F32 = jnp.float32
BF16 = jnp.bfloat16
NK = 8
NE = 8
CAP = 8
PAIR_OF = (0, 2, 1, 4, 3, 6, 5, 7)
GROUPS = ((0, 2), (2, 2), (4, 2), (6, 2))


def scoped(f):
    @functools.wraps(f)
    def run(*args):
        with jax.named_scope(f.__name__):
            return f(*args)

    return run


def dot_last(a, b):
    return lax.dot_general(a, b, (((1,), (1,)), ((), ())), preferred_element_type=F32)


def dot_first(a, b):
    return lax.dot_general(a, b, (((0,), (0,)), ((), ())), preferred_element_type=F32)


def dot(a, b):
    return jnp.dot(a, b, preferred_element_type=F32)


def step_kernel(
    tok_hbm,
    grad_hbm,
    ids_hbm,
    rw_hbm,
    wg_hbm,
    wu_hbm,
    wd_hbm,
    tg_ref,
    rg_ref,
    gg_ref,
    ug_ref,
    dg_ref,
    tokv,
    idsv,
    rwv,
    wg,
    wu,
    wd,
    zbuf,
    tiles,
    etiles,
    codes,
    pcodes,
    upper,
    transit,
    pbuf,
    ysend,
    buf,
    dgu,
    wtd,
    dxq,
    r1,
    acc,
    s2,
    r2,
    yret,
    yrr,
    wsend,
    wrecv,
    sx,
    sy,
    syr,
    szs,
    smat,
    dmat,
    means,
    dys,
    de,
    ld,
    sent,
    got,
    zrs,
    irs,
    ers,
    trs,
    yrs,
    xrs,
    r1r,
    r2r,
    vrs,
):
    ep = lax.axis_index("ep")
    x = lax.axis_index("tp")
    z = ep // NE
    yc = ep % NE
    y = yc // 2
    core = yc % 2
    par = x % 2
    odd = x % 2
    near_a = x + 1 - 2 * odd
    near_b = (x + 3 + 2 * odd) % 4
    far = (x + 2) % 4
    right = (x + 1) % 4
    left = (x + 3) % 4

    def remote(src, dst, ss, rs, e, t):
        return pltpu.make_async_remote_copy(
            src_ref=src,
            dst_ref=dst,
            send_sem=ss,
            recv_sem=rs,
            device_id={"ep": e, "tp": t},
            device_id_type=MESH,
        )

    def arrived(ref, sem):
        pltpu.make_async_copy(ref, ref, sem).wait()

    def z_of(k):
        h = (k + 1) // 2
        s = 1 - 2 * ((k + 1) % 2)
        return (z + s * h + NK) % NK

    def at_z(zz):
        return zz * NE + yc

    def at_e(j):
        return z * NE + j

    def in_plane(dy, c):
        return ((y + dy + 4) % 4) * 2 + c

    barrier = pltpu.get_barrier_semaphore()
    for d in (1, NK - 1):
        pl.semaphore_signal(
            barrier, inc=1, device_id={"ep": at_z((z + d) % NK), "tp": x}, device_id_type=MESH
        )
    for d in range(1, NE):
        pl.semaphore_signal(
            barrier, inc=1, device_id={"ep": at_e((yc + d) % NE), "tp": x}, device_id_type=MESH
        )
    for d in range(1, 4):
        pl.semaphore_signal(
            barrier, inc=1, device_id={"ep": ep, "tp": (x + d) % 4}, device_id_type=MESH
        )

    load_tok = pltpu.make_async_copy(tok_hbm, tokv, ld.at[0])
    load_tok.start()
    load_ids = pltpu.make_async_copy(ids_hbm, idsv, ld.at[5])
    load_rw = pltpu.make_async_copy(rw_hbm, rwv, ld.at[6])
    load_ids.start()
    load_rw.start()

    @pl.when(par == 0)
    def _():
        pltpu.make_async_copy(tok_hbm, zbuf.at[0], ld.at[1]).start()

    @pl.when(par == 1)
    def _():
        pltpu.make_async_copy(grad_hbm, zbuf.at[0], ld.at[1]).start()

    load_g = pltpu.make_async_copy(wg_hbm, wg, ld.at[2])
    load_u = pltpu.make_async_copy(wu_hbm, wu, ld.at[3])
    load_d = pltpu.make_async_copy(wd_hbm, wd, ld.at[4])
    load_g.start()
    load_u.start()
    load_d.start()

    @scoped
    def wait_small():
        load_tok.wait()
        load_ids.wait()
        load_rw.wait()

    wait_small()
    n_tok = tokv.shape[0]
    n_exp = rwv.shape[0]
    logits = dot_last(rwv[...], tokv[...])
    expert = lax.broadcasted_iota(jnp.int32, (n_exp, n_tok), 0)
    picked = []
    for k in range(idsv.shape[0]):
        here = idsv[k : k + 1, :] == expert
        picked.append(jnp.sum(jnp.where(here, logits, 0.0), axis=0, keepdims=True))
    picked = jnp.concatenate(picked, axis=0)
    expd = jnp.exp(picked - jnp.max(picked, axis=0, keepdims=True))
    gates = expd / jnp.sum(expd, axis=0, keepdims=True)
    tiles[0] = jnp.full((8, 128), -1.0, F32)
    tiles[0, 0:4, 0:n_tok] = idsv[...].astype(F32)
    tiles[0, 4:8, 0:n_tok] = gates
    row = lax.broadcasted_iota(jnp.int32, (128, 128), 0)
    col = lax.broadcasted_iota(jnp.int32, (128, 128), 1)
    upper[...] = jnp.where(row < col, 1.0, 0.0).astype(BF16)

    def rank_of(hit):
        return jnp.where(hit > 0.0, dot(hit.astype(BF16), upper[...]), -1.0)

    def codes_of(tile, first, count):
        experts = (lax.broadcasted_iota(jnp.int32, (count, 128), 0) + first).astype(F32)
        hit = jnp.zeros((count, 128), F32)
        gate = jnp.zeros((count, 128), F32)
        for k in range(4):
            here = tile[k : k + 1, :] == experts
            hit = hit + jnp.where(here, 1.0, 0.0)
            gate = gate + jnp.where(here, tile[4 + k : 5 + k, :], 0.0)
        return rank_of(hit), gate

    @scoped
    def wait_barrier():
        pl.semaphore_wait(barrier, 2 + (NE - 1) + 3)

    wait_barrier()

    pltpu.make_async_copy(tok_hbm, zbuf.at[0], ld.at[1]).wait()

    half = zbuf.shape[2] // 2

    def z_copy(k, part):
        to = 7 if k >= 5 else k + 2
        s = 1 - 2 * ((k + 1) % 2)
        cols = pl.ds(part * half, half)
        return remote(
            zbuf.at[k, :, cols],
            zbuf.at[to, :, cols],
            sent.at[0],
            zrs.at[to, part],
            at_z((z - s + NK) % NK),
            x,
        )

    def z_first(part, way):
        cols = pl.ds(part * half, half)
        return remote(
            zbuf.at[0, :, cols],
            zbuf.at[1 + way, :, cols],
            sent.at[0],
            zrs.at[1 + way, part],
            at_z((z + 1) % NK) if way else at_z((z + NK - 1) % NK),
            x,
        )

    def tile_copy(k):
        s = 1 - 2 * ((k + 1) % 2)
        return remote(
            tiles.at[k], tiles.at[k + 2], sent.at[1], irs.at[k + 2], at_z((z - s + NK) % NK), x
        )

    below, above = at_z((z + NK - 1) % NK), at_z((z + 1) % NK)
    t_left = remote(tiles.at[0], tiles.at[1], sent.at[1], irs.at[1], below, x)
    t_right = remote(tiles.at[0], tiles.at[2], sent.at[1], irs.at[2], above, x)
    t_left.start()
    t_right.start()
    for part in range(2):
        for way in range(2):
            z_first(part, way).start()

    def share_copy(k, d):
        j = (yc + d) % NE
        return remote(
            tiles.at[k],
            etiles.at[k, pl.ds(pl.multiple_of(yc * 8, 8), 8)],
            sent.at[2],
            ers.at[k],
            at_e(j),
            x,
        )

    def share_wait(k):
        arrived(etiles.at[k, pl.ds(0, 8 * (NE - 1))], ers.at[k])

    steps = ((1, 0), (1, 1), (-1, 0), (-1, 1))

    def transit_copy(k, way):
        e = in_plane(2, way)
        return remote(
            ysend.at[k, e],
            transit.at[k, way],
            sent.at[3],
            trs.at[k],
            at_e(in_plane(-1 if way else 1, core)),
            x,
        )

    def near_copy(k, n):
        j = in_plane(*steps[n]) if n < 4 else in_plane(0, 1 - core)
        return remote(
            ysend.at[k, j], buf.at[par, k * NE + yc], sent.at[4], yrs.at[k], at_e(j), x
        )

    def forward_copy(k, way):
        src = in_plane(1 if way else -1, core)
        return remote(
            transit.at[k, way],
            buf.at[par, k * NE + src],
            sent.at[3],
            yrs.at[k],
            at_e(in_plane(-1 if way else 1, way)),
            x,
        )

    @scoped
    def take(k, part):
        if part == 0:
            arrived(tiles.at[k], irs.at[k])
            if k <= 5:
                tile_copy(k).start()
        cols = pl.ds(part * half, half)
        arrived(zbuf.at[k, :, cols], zrs.at[k, part])
        if k <= 4 or (k, part) in ((5, 1), (6, 0)):
            z_copy(k, part).start()

    @scoped
    def select_block(k):
        for d in range(1, NE):
            share_copy(k, d).start()
        tile = tiles[k]
        etiles[k, pl.ds(pl.multiple_of(yc * 8, 8), 8)] = tile
        code, gate = codes_of(tile, z * NE, NE)
        pcodes[0, k] = code
        pcodes[1, k] = gate
        want = lax.broadcasted_iota(jnp.int32, (NE, CAP, 128), 1).astype(F32)
        place = (jnp.broadcast_to(code[:, None, :], (NE, CAP, 128)) == want).astype(F32)
        place = place.reshape(NE * CAP, 128).astype(BF16)
        pbuf[k] = place
        block = zbuf[k]
        for q in range(4):
            cols = slice(512 * q, 512 * (q + 1))
            rows = dot(place[:, 0:n_tok], block[:, cols])
            ysend[k, :, :, cols] = rows.astype(BF16).reshape(NE, CAP, 512)
        transit_copy(k, 0).start()
        transit_copy(k, 1).start()
        for n in (0, 2, 1, 3, 4):
            near_copy(k, n).start()
        buf[par, k * NE + yc] = ysend[k, yc]

    @scoped
    def hand_over(k):
        arrived(transit.at[k], trs.at[k])
        for way in range(2):
            forward_copy(k, way).start()

    half_e = NE // 2

    def x_copy(k, side):
        rows = pl.ds(k * NE + side * half_e, half_e)
        return remote(
            buf.at[par, rows],
            buf.at[par, rows],
            sent.at[5],
            xrs.at[k],
            ep,
            left if side else right,
        )

    @scoped
    def x_waits(k):
        arrived(buf.at[1 - par, pl.ds(k * NE, NE)], xrs.at[k])

    @scoped
    def y_waits(k):
        arrived(buf.at[par, pl.ds(k * NE, NE - 1)], yrs.at[k])

    @scoped
    def pass_on(k):
        y_waits(k)
        x_copy(k, 0).start()
        x_copy(k, 1).start()

    def slot_info(k):
        hit = jnp.zeros((NE, 128), F32)
        gate = jnp.zeros((NE, 128), F32)
        mine = ep.astype(F32)
        for c in range(4):
            here = etiles[k, pl.ds(c, NE, stride=8), :] == mine
            hit = hit + jnp.where(here, 1.0, 0.0)
            gate = gate + jnp.where(here, etiles[k, pl.ds(4 + c, NE, stride=8), :], 0.0)
        return rank_of(hit), gate

    def score_copy(m, d):
        t = (x + d) % 4
        rows = pl.ds(GROUPS[m][0] * NE, GROUPS[m][1] * NE)
        return remote(sx.at[0, rows], sx.at[4 - d, rows], sent.at[6], got.at[0], ep, t)

    def unit(m, which):
        k, n = GROUPS[m]
        return pl.ds(k * NE + which * n * NE // 2, n * NE // 2)

    def halves_copy(m, which, slot):
        peer = near_b if which else near_a
        q = far if slot else peer
        rows = unit(m, which)
        return remote(
            dxq.at[q, rows], r1.at[slot, rows], sent.at[7], r1r.at[m, slot], ep, peer
        )

    def group(m):
        k, n = GROUPS[m]
        return pl.ds(k * NE, n * NE)

    @scoped
    def compute(m):
        first, count = GROUPS[m]
        n_rows = count * NE * CAP
        infos = []
        for k in range(first, first + count):
            share_wait(k)
            infos.append(slot_info(k))
            codes[0, k], codes[1, k] = infos[-1]
        code = jnp.concatenate([i[0] for i in infos], axis=0)
        gate = jnp.concatenate([i[1] for i in infos], axis=0)
        shape = (count * NE, CAP, 128)
        want = lax.broadcasted_iota(jnp.int32, shape, 1).astype(F32)
        mine = jnp.broadcast_to(code[:, None, :], shape) == want
        wide = jnp.where(mine, jnp.broadcast_to(gate[:, None, :], shape), 0.0)
        weight = jnp.sum(wide.reshape(n_rows, 128), axis=1, keepdims=True)
        for k in range(first, first + count):
            x_waits(k)
        rows = pl.ds(first * NE, count * NE)
        flat = pl.ds(first * NE * CAP, n_rows)
        xin = buf[0, rows].reshape(n_rows, 2048)
        gin = buf[1, rows].reshape(n_rows, 2048)
        gate_pre = dot(xin, wg[...])
        up_pre = dot(xin, wu[...])
        back = dot_last(gin, wd[...])
        glu = jnp.minimum(gate_pre, 7.0)
        lin1 = jnp.clip(up_pre, -7.0, 7.0) + 1.0
        sig = jax.nn.sigmoid(1.702 * glu)
        act = glu * sig
        hidden = lin1 * act
        slope = lin1 * (sig + 1.702 * glu * sig * (1.0 - sig))
        slope = jnp.where(gate_pre < 7.0, slope, 0.0)
        up_slope = jnp.where((up_pre > -7.0) & (up_pre < 7.0), act, 0.0)
        score = jnp.sum(hidden * back, axis=1, keepdims=True)
        d_hidden = weight * back
        d_gate = (d_hidden * slope).astype(BF16)
        d_up = (d_hidden * up_slope).astype(BF16)
        dgu[flat, 0:384] = d_gate
        dgu[flat, 384:768] = d_up
        wtd[flat, :] = (weight * hidden).astype(BF16)
        lane = lax.broadcasted_iota(jnp.int32, shape, 2)
        sub = lax.broadcasted_iota(jnp.int32, shape, 1)
        spread = jnp.broadcast_to(score, (n_rows, 128)).reshape(shape)
        sx[0, rows] = jnp.sum(jnp.where(lane == sub, spread, 0.0), axis=1)
        for d in range(1, 4):
            score_copy(m, d).start()

        for q in range(4):
            cols = slice(512 * q, 512 * (q + 1))
            part = dot_last(d_gate, wg[cols, :]) + dot_last(d_up, wu[cols, :])
            dxq[q, rows] = part.astype(BF16).reshape(count * NE, CAP, 512)
        for slot in (1, 0):
            for which in range(2):
                halves_copy(m, which, slot).start()

    def quarter_copy(m, which):
        rows = unit(m, which)
        return remote(
            s2.at[rows], r2.at[rows], sent.at[8], r2r.at[m], ep, near_a if which else near_b
        )

    @scoped
    def wait_half(m, slot):
        arrived(r1.at[slot, group(m)], r1r.at[m, slot])

    @scoped
    def wait_quarter(m):
        arrived(r2.at[group(m)], r2r.at[m])

    @scoped
    def reduce_first(m):
        wait_half(m, 1)
        for which in range(2):
            rows = unit(m, which)
            s2[rows] = (
                dxq[near_a if which else near_b, rows].astype(F32) + r1[1, rows].astype(F32)
            ).astype(BF16)
            quarter_copy(m, which).start()
        wait_half(m, 0)
        for which in range(2):
            rows = unit(m, which)
            acc[rows] = dxq[x, rows].astype(F32) + r1[0, rows].astype(F32)

    def back_copy(m, d):
        j = (yc + d) % NE
        ks = pl.ds(*GROUPS[m])
        return remote(yret.at[j, ks], yrr.at[yc, ks], sent.at[9], vrs.at[m], at_e(j), x)

    @scoped
    def reduce_second(m):
        first, count = GROUPS[m]
        wait_quarter(m)
        for k in range(first, first + count):
            rows = pl.ds(k * NE, NE)
            total = (acc[rows] + r2[rows].astype(F32)).astype(BF16)
            for j in range(NE):
                yret[j, k] = total[j]
        for d in (1, 7, 2, 6, 3, 5, 4):
            back_copy(m, d).start()
        ks = pl.ds(first, count)
        yrr[yc, ks] = yret[yc, ks]

    def home_copy(k):
        return remote(
            wsend.at[k], wrecv.at[PAIR_OF[k]], sent.at[10], got.at[1], at_z(z_of(k)), x
        )

    @scoped
    def back_waits(m):
        arrived(yrr.at[pl.ds(0, NE - 1), pl.ds(*GROUPS[m])], vrs.at[m])

    @scoped
    def combine(m):
        back_waits(m)
        first, count = GROUPS[m]
        for k in range(first, first + count):
            rows = jnp.concatenate([yrr[j, k] for j in range(NE)], axis=0)
            wsend[k] = dot_first(pbuf[k][:, 0:n_tok], rows).astype(BF16)
            if k > 0:
                home_copy(k).start()

    def both(f, *ks):
        for k in ks:
            f(k)

    def takes(part, *ks):
        for k in ks:
            take(k, part)

    select_block(0)
    takes(0, 1, 2)
    hand_over(0)
    takes(1, 1, 2)
    select_block(1)
    select_block(2)
    pass_on(0)
    takes(0, 3, 4)
    hand_over(1)
    takes(1, 3, 4)
    select_block(3)
    hand_over(2)
    pass_on(1)
    select_block(4)
    takes(0, 5, 6)
    hand_over(3)
    pass_on(2)
    takes(1, 5, 6)
    select_block(5)
    hand_over(4)
    pass_on(3)
    select_block(6)
    take(7, 0)
    take(7, 1)
    load_g.wait()
    load_u.wait()
    load_d.wait()
    compute(0)
    hand_over(5)
    pass_on(4)
    select_block(7)
    hand_over(6)
    pass_on(5)
    compute(1)
    hand_over(7)
    pass_on(6)
    pass_on(7)
    reduce_first(0)
    compute(2)
    reduce_first(1)
    compute(3)
    reduce_second(0)

    @scoped
    def weight_tile(i, carry):
        cols = pl.ds(pl.multiple_of(i * 256, 256), 256)
        xs = buf[0, :, :, cols].reshape(512, 256)
        both = dot_first(xs, dgu[...]).astype(BF16)
        gg_ref[cols, :] = both[:, 0:384]
        ug_ref[cols, :] = both[:, 384:768]
        gs = buf[1, :, :, cols].reshape(512, 256)
        dg_ref[:, cols] = dot_first(wtd[...], gs).astype(BF16)
        return carry

    def weight_tiles(a, b):
        lax.fori_loop(a, b, weight_tile, 0)

    def sy_copy(d):
        j = (yc + d) % NE
        return remote(sy.at[j], syr.at[yc], sent.at[11], got.at[2], at_e(j), x)

    @scoped
    def scores_x():
        arrived(sx.at[pl.ds(1, 3)], got.at[0])
        sx[1] = (sx[0] + sx[1]) + (sx[2] + sx[3])
        for j in range(NE):
            sy[j] = jnp.concatenate(
                [sx[1, k * NE + j : k * NE + j + 1, :] for k in range(NK)], axis=0
            )
        for d in range(1, NE):
            sy_copy(d).start()
        syr[yc] = sy[yc]

    def sz_copy(k):
        return remote(
            szs.at[k],
            smat.at[pl.ds(pl.multiple_of(z * NE, NE), NE)],
            sent.at[12],
            got.at[3],
            at_z(z_of(k)),
            x,
        )

    def mean_copy(k):
        return remote(
            means.at[0],
            means.at[PAIR_OF[k]],
            sent.at[13],
            got.at[4],
            at_z(z_of(k)),
            x,
        )

    def at_ranks(code, scores):
        found = jnp.zeros(code.shape, F32)
        for r in range(CAP):
            found = found + jnp.where(code == float(r), scores[:, r : r + 1], 0.0)
        return found

    @scoped
    def scores_y():
        arrived(syr.at[pl.ds(0, NE - 1)], got.at[2])
        for k in range(NK):
            szs[k] = jnp.concatenate([syr[e, k : k + 1, :] for e in range(NE)], axis=0)
            part = pcodes[1, k] * at_ranks(pcodes[0, k], szs[k])
            means[0, pl.ds(z_of(k), 1), :] = jnp.sum(part, axis=0, keepdims=True)
        for k in range(1, NK):
            mean_copy(k).start()
        for k in range(1, NK):
            sz_copy(k).start()
        smat[pl.ds(pl.multiple_of(z * NE, NE), NE), :] = szs[0]

    def dy_copy(d):
        j = (yc + d) % NE
        return remote(dys, de.at[yc], sent.at[14], got.at[5], at_e(j), x)

    @scoped
    def scores_z():
        arrived(means.at[pl.ds(1, NK - 1)], got.at[4])
        total = means[0]
        for k in range(1, NK):
            total = total + means[k]
        dys[...] = total
        for d in range(1, NE):
            dy_copy(d).start()
        de[yc] = total

    @scoped
    def home_logits():
        arrived(smat.at[pl.ds(0, NE * (NK - 1))], got.at[3])
        code_t, gate_t = codes_of(tiles[0], 0, n_exp)
        score_at = at_ranks(code_t, smat)
        mean = jnp.sum(gate_t * score_at, axis=0, keepdims=True)
        dmat[...] = jnp.where(code_t >= 0.0, gate_t * (score_at - mean), 0.0)

    x_rows = pl.ds(pl.multiple_of(x * 512, 512), 512)

    @scoped
    def token_out():
        d_t = dmat[...]
        d_hi = d_t.astype(BF16)
        d_lo = (d_t - d_hi.astype(F32)).astype(BF16)
        rw_x = rwv[:, x_rows]
        total = (dot_first(d_hi, rw_x) + dot_first(d_lo, rw_x))[0:n_tok, :]
        total = total + wsend[0].astype(F32)
        arrived(wrecv.at[pl.ds(1, NK - 1)], got.at[1])
        for k in range(1, NK):
            total = total + wrecv[k].astype(F32)
        tg_ref[...] = total.astype(BF16)

    @scoped
    def router_out():
        arrived(de.at[pl.ds(0, NE - 1)], got.at[5])
        shape = (NE, CAP, 128)
        want = lax.broadcasted_iota(jnp.int32, shape, 1).astype(F32)
        lane = lax.broadcasted_iota(jnp.int32, shape, 2)
        sub = lax.broadcasted_iota(jnp.int32, shape, 1)
        sums = jnp.zeros((CAP, 512), F32)

        def of_slots(mask, rows):
            wide = jnp.where(mask, jnp.broadcast_to(rows[:, None, :], shape), 0.0)
            return jnp.sum(wide, axis=2, keepdims=True)

        for k in range(NK):
            mean = jnp.concatenate([de[j, pl.ds(z_of(k), 1), :] for j in range(NE)], axis=0)
            code, gate = codes[0, k], codes[1, k]
            mine = jnp.broadcast_to(code[:, None, :], shape) == want
            score = of_slots(lane == sub, sx[1, k * NE : (k + 1) * NE, :])
            slot_d = of_slots(mine, gate) * (score - of_slots(mine, mean))
            rows = buf[0, k * NE : (k + 1) * NE, :, x_rows].astype(F32)
            sums = sums + jnp.sum(slot_d * rows, axis=0)
        rg_ref[...] = jnp.sum(sums, axis=0, keepdims=True)

    reduce_second(1)
    reduce_first(2)
    weight_tiles(0, 1)
    scores_x()
    combine(0)
    weight_tiles(1, 2)
    reduce_first(3)
    combine(1)
    reduce_second(2)
    scores_y()
    weight_tiles(2, 3)
    reduce_second(3)
    combine(2)
    weight_tiles(3, 5)
    combine(3)
    scores_z()
    weight_tiles(5, 8)
    home_logits()
    router_out()
    token_out()

    with jax.named_scope("drain_all"):
        seven = pl.ds(0, 7)
        for i, ref in enumerate(
            (
                zbuf.at[seven],
                tiles.at[seven],
                etiles.at[seven, pl.ds(0, 64)],
                ysend.at[pl.ds(0, 4)],
                ysend.at[pl.ds(0, 5)],
                buf.at[0],
                sx.at[pl.ds(0, 3)],
                r1,
                s2,
                yret.at[seven],
                wsend.at[seven],
                sy.at[seven],
                szs.at[seven],
                means.at[seven],
                means.at[seven],
            )
        ):
            arrived(ref, sent.at[i])


def finish_kernel(tg, rg, gg, ug, dg, tg_o, rg_o, gg_o, ug_o, dg_o, sems):
    pairs = ((gg, gg_o), (ug, ug_o), (dg, dg_o), (tg, tg_o), (rg, rg_o))
    copies = [pltpu.make_async_copy(a, b, sems.at[i]) for i, (a, b) in enumerate(pairs)]
    for c in copies:
        c.start()
    for c in copies:
        c.wait()


def per_device(tokens, out_grad, expert_ids, router_weight, w_gate, w_up, w_down):
    n_tok, width = tokens.shape
    n_exp = router_weight.shape[1]
    top_count = expert_ids.shape[1]
    ff = w_gate.shape[2]
    quarter = width // 4
    any_space = pl.BlockSpec(memory_space=pl.ANY)
    vmem = pl.BlockSpec(memory_space=pltpu.VMEM)
    hbm = pl.BlockSpec(memory_space=pltpu.HBM)
    dma = pltpu.SemaphoreType.DMA
    slots = NK * NE
    scratch = [
        pltpu.VMEM((n_tok, width), BF16),
        pltpu.VMEM((top_count, n_tok), jnp.int32),
        pltpu.VMEM((n_exp, width), BF16),
        pltpu.VMEM((width, ff), BF16),
        pltpu.VMEM((width, ff), BF16),
        pltpu.VMEM((ff, width), BF16),
        pltpu.VMEM((NK, n_tok, width), BF16),
        pltpu.VMEM((NK, 8, 128), F32),
        pltpu.VMEM((NK, NE * 8, 128), F32),
        pltpu.VMEM((2, NK, NE, 128), F32),
        pltpu.VMEM((2, NK, NE, 128), F32),
        pltpu.VMEM((128, 128), BF16),
        pltpu.VMEM((NK, 2, CAP, width), BF16),
        pltpu.VMEM((NK, NE * CAP, 128), BF16),
        pltpu.VMEM((NK, NE, CAP, width), BF16),
        pltpu.VMEM((2, slots, CAP, width), BF16),
        pltpu.VMEM((slots * CAP, 2 * ff), BF16),
        pltpu.VMEM((slots * CAP, ff), BF16),
        pltpu.VMEM((4, slots, CAP, quarter), BF16),
        pltpu.VMEM((2, slots, CAP, quarter), BF16),
        pltpu.VMEM((slots, CAP, quarter), F32),
        pltpu.VMEM((slots, CAP, quarter), BF16),
        pltpu.VMEM((slots, CAP, quarter), BF16),
        pltpu.VMEM((NE, NK, CAP, quarter), BF16),
        pltpu.VMEM((NE, NK, CAP, quarter), BF16),
        pltpu.VMEM((NK, n_tok, quarter), BF16),
        pltpu.VMEM((NK, n_tok, quarter), BF16),
        pltpu.VMEM((4, slots, 128), F32),
        pltpu.VMEM((NE, NK, 128), F32),
        pltpu.VMEM((NE, NK, 128), F32),
        pltpu.VMEM((NK, NE, 128), F32),
        pltpu.VMEM((n_exp, 128), F32),
        pltpu.VMEM((n_exp, 128), F32),
        pltpu.VMEM((NK, NK, 128), F32),
        pltpu.VMEM((NK, 128), F32),
        pltpu.VMEM((NE, NK, 128), F32),
        dma((7,)),
        dma((15,)),
        dma((6,)),
        dma((8, 2)),
        dma((8,)),
        dma((8,)),
        dma((8,)),
        dma((8,)),
        dma((8,)),
        dma((4, 2)),
        dma((4,)),
        dma((4,)),
    ]
    shapes = (
        jax.ShapeDtypeStruct((n_tok, quarter), BF16),
        jax.ShapeDtypeStruct((1, quarter), F32),
        jax.ShapeDtypeStruct((width, ff), BF16),
        jax.ShapeDtypeStruct((width, ff), BF16),
        jax.ShapeDtypeStruct((ff, width), BF16),
    )
    out = pl.pallas_call(
        step_kernel,
        name="moe_backward",
        out_shape=shapes,
        in_specs=[hbm] * 7,
        out_specs=(vmem,) * 5,
        scratch_shapes=scratch,
        compiler_params=pltpu.CompilerParams(
            collective_id=0, has_side_effects=True, vmem_limit_bytes=40 * 1024 * 1024
        ),
    )(
        *(
            pltpu.with_memory_space_constraint(a, pltpu.HBM)
            for a in (
                tokens,
                out_grad,
                expert_ids.T,
                router_weight.T,
                w_gate[0],
                w_up[0],
                w_down[0],
            )
        )
    )
    token_grad, router_grad, gate_grad, up_grad, down_grad = pl.pallas_call(
        finish_kernel,
        name="finish",
        out_shape=shapes,
        in_specs=[any_space] * 5,
        out_specs=(any_space,) * 5,
        scratch_shapes=[dma((5,))],
        compiler_params=pltpu.CompilerParams(vmem_limit_bytes=4 * 1024 * 1024),
    )(*out)
    return (
        token_grad,
        router_grad.reshape(quarter, 1),
        gate_grad[None],
        up_grad[None],
        down_grad[None],
    )


def solution(mesh):
    in_specs = (
        P("ep", None),
        P("ep", None),
        P("ep", None),
        P(),
        P("ep", None, "tp"),
        P("ep", None, "tp"),
        P("ep", "tp", None),
    )
    out_specs = (
        P("ep", "tp"),
        P("tp", "ep"),
        P("ep", None, "tp"),
        P("ep", None, "tp"),
        P("ep", "tp", None),
    )
    return jax.shard_map(
        per_device, mesh=mesh, in_specs=in_specs, out_specs=out_specs, check_vma=False
    )
```

```python
import functools

import jax
import jax.numpy as jnp
from jax import lax
from jax.experimental import pallas as pl
from jax.experimental.pallas import tpu as pltpu
from jax.sharding import PartitionSpec as P

MESH = pl.DeviceIdType.MESH
F32 = jnp.float32
BF16 = jnp.bfloat16
NK = 8
NE = 8
CAP = 8
PAIR_OF = (0, 2, 1, 4, 3, 6, 5, 7)
GROUPS = ((0, 2), (2, 2), (4, 2), (6, 2))
DIRECT = (1, 2)


def place_of(k):
    return (k + NK - 1) % NK


def block_at(n):
    return (n + 1) % NK


def scoped(f):
    @functools.wraps(f)
    def run(*args):
        with jax.named_scope(f.__name__):
            return f(*args)

    return run


def dot_last(a, b):
    return lax.dot_general(a, b, (((1,), (1,)), ((), ())), preferred_element_type=F32)


def dot_first(a, b):
    return lax.dot_general(a, b, (((0,), (0,)), ((), ())), preferred_element_type=F32)


def dot(a, b):
    return jnp.dot(a, b, preferred_element_type=F32)


def step_kernel(
    tok_hbm,
    grad_hbm,
    ids_hbm,
    rw_hbm,
    wg_hbm,
    wu_hbm,
    wd_hbm,
    tg_ref,
    rg_ref,
    gg_ref,
    ug_ref,
    dg_ref,
    tokv,
    idsv,
    rwv,
    wg,
    wu,
    wd,
    zbuf,
    tiles,
    etiles,
    codes,
    pcodes,
    upper,
    transit,
    pbuf,
    ysend,
    buf,
    dgu,
    wtd,
    dxq,
    r1,
    acc,
    s2,
    r2,
    yret,
    yrr,
    wsend,
    wrecv,
    sx,
    sy,
    syr,
    szs,
    smat,
    dmat,
    means,
    dys,
    de,
    ld,
    sent,
    got,
    zrs,
    irs,
    ers,
    trs,
    yrs,
    xrs,
    r1r,
    r2r,
    vrs,
):
    ep = lax.axis_index("ep")
    x = lax.axis_index("tp")
    z = ep // NE
    yc = ep % NE
    y = yc // 2
    core = yc % 2
    par = x % 2
    odd = x % 2
    near_a = x + 1 - 2 * odd
    near_b = (x + 3 + 2 * odd) % 4
    far = (x + 2) % 4
    right = (x + 1) % 4
    left = (x + 3) % 4

    def remote(src, dst, ss, rs, e, t):
        return pltpu.make_async_remote_copy(
            src_ref=src,
            dst_ref=dst,
            send_sem=ss,
            recv_sem=rs,
            device_id={"ep": e, "tp": t},
            device_id_type=MESH,
        )

    def arrived(ref, sem):
        pltpu.make_async_copy(ref, ref, sem).wait()

    def z_of(k):
        h = (k + 1) // 2
        s = 1 - 2 * ((k + 1) % 2)
        return (z + s * h + NK) % NK

    def at_z(zz):
        return zz * NE + yc

    def at_e(j):
        return z * NE + j

    def in_plane(dy, c):
        return ((y + dy + 4) % 4) * 2 + c

    barrier = pltpu.get_barrier_semaphore()
    for d in (1, NK - 1):
        pl.semaphore_signal(
            barrier, inc=1, device_id={"ep": at_z((z + d) % NK), "tp": x}, device_id_type=MESH
        )
    for d in range(1, NE):
        pl.semaphore_signal(
            barrier, inc=1, device_id={"ep": at_e((yc + d) % NE), "tp": x}, device_id_type=MESH
        )
    for d in range(1, 4):
        pl.semaphore_signal(
            barrier, inc=1, device_id={"ep": ep, "tp": (x + d) % 4}, device_id_type=MESH
        )

    load_tok = pltpu.make_async_copy(tok_hbm, tokv, ld.at[0])
    load_tok.start()
    load_ids = pltpu.make_async_copy(ids_hbm, idsv, ld.at[5])
    load_rw = pltpu.make_async_copy(rw_hbm, rwv, ld.at[6])
    load_ids.start()
    load_rw.start()

    @pl.when(par == 0)
    def _():
        pltpu.make_async_copy(tok_hbm, zbuf.at[0], ld.at[1]).start()

    @pl.when(par == 1)
    def _():
        pltpu.make_async_copy(grad_hbm, zbuf.at[0], ld.at[1]).start()

    load_g = pltpu.make_async_copy(wg_hbm, wg, ld.at[2])
    load_u = pltpu.make_async_copy(wu_hbm, wu, ld.at[3])
    load_d = pltpu.make_async_copy(wd_hbm, wd, ld.at[4])
    load_g.start()
    load_u.start()
    load_d.start()

    @scoped
    def wait_small():
        load_tok.wait()
        load_ids.wait()
        load_rw.wait()

    @scoped
    def wait_barrier():
        pl.semaphore_wait(barrier, 2 + (NE - 1) + 3)

    wait_barrier()

    pltpu.make_async_copy(tok_hbm, zbuf.at[0], ld.at[1]).wait()

    half = zbuf.shape[2] // 2

    def z_copy(k, part):
        to = 7 if k >= 5 else k + 2
        s = 1 - 2 * ((k + 1) % 2)
        cols = pl.ds(part * half, half)
        return remote(
            zbuf.at[k, :, cols],
            zbuf.at[to, :, cols],
            sent.at[0],
            zrs.at[to, part],
            at_z((z - s + NK) % NK),
            x,
        )

    def z_first(part, way):
        cols = pl.ds(part * half, half)
        return remote(
            zbuf.at[0, :, cols],
            zbuf.at[1 + way, :, cols],
            sent.at[0],
            zrs.at[1 + way, part],
            at_z((z + 1) % NK) if way else at_z((z + NK - 1) % NK),
            x,
        )

    def tile_copy(k):
        s = 1 - 2 * ((k + 1) % 2)
        return remote(
            tiles.at[k], tiles.at[k + 2], sent.at[1], irs.at[k + 2], at_z((z - s + NK) % NK), x
        )

    below, above = at_z((z + NK - 1) % NK), at_z((z + 1) % NK)
    t_left = remote(tiles.at[0], tiles.at[1], sent.at[1], irs.at[1], below, x)
    t_right = remote(tiles.at[0], tiles.at[2], sent.at[1], irs.at[2], above, x)
    z_first(0, 0).start()
    z_first(0, 1).start()
    wait_small()
    n_tok = tokv.shape[0]
    n_exp = rwv.shape[0]
    logits = dot_last(rwv[...], tokv[...])
    expert = lax.broadcasted_iota(jnp.int32, (n_exp, n_tok), 0)
    picked = []
    for k in range(idsv.shape[0]):
        here = idsv[k : k + 1, :] == expert
        picked.append(jnp.sum(jnp.where(here, logits, 0.0), axis=0, keepdims=True))
    picked = jnp.concatenate(picked, axis=0)
    expd = jnp.exp(picked - jnp.max(picked, axis=0, keepdims=True))
    gates = expd / jnp.sum(expd, axis=0, keepdims=True)
    tiles[0] = jnp.full((8, 128), -1.0, F32)
    tiles[0, 0:4, 0:n_tok] = idsv[...].astype(F32)
    tiles[0, 4:8, 0:n_tok] = gates
    row = lax.broadcasted_iota(jnp.int32, (128, 128), 0)
    col = lax.broadcasted_iota(jnp.int32, (128, 128), 1)
    upper[...] = jnp.where(row < col, 1.0, 0.0).astype(BF16)

    def rank_of(hit):
        return jnp.where(hit > 0.0, dot(hit.astype(BF16), upper[...]), -1.0)

    def codes_of(tile, first, count):
        experts = (lax.broadcasted_iota(jnp.int32, (count, 128), 0) + first).astype(F32)
        hit = jnp.zeros((count, 128), F32)
        gate = jnp.zeros((count, 128), F32)
        for k in range(4):
            here = tile[k : k + 1, :] == experts
            hit = hit + jnp.where(here, 1.0, 0.0)
            gate = gate + jnp.where(here, tile[4 + k : 5 + k, :], 0.0)
        return rank_of(hit), gate

    t_left.start()
    t_right.start()
    z_first(1, 0).start()
    z_first(1, 1).start()

    def share_copy(k, d):
        j = (yc + d) % NE
        return remote(
            tiles.at[k],
            etiles.at[k, pl.ds(pl.multiple_of(yc * 8, 8), 8)],
            sent.at[2],
            ers.at[k],
            at_e(j),
            x,
        )

    def share_wait(k):
        arrived(etiles.at[k, pl.ds(0, 8 * (NE - 1))], ers.at[k])

    steps = ((1, 0), (1, 1), (-1, 0), (-1, 1))

    def transit_copy(k, way, cols):
        e = in_plane(2, way)
        return remote(
            ysend.at[k, e],
            transit.at[k, way],
            sent.at[3],
            trs.at[k],
            at_e(in_plane(-1 if way else 1, core)),
            x,
        )

    def direct_copy(k, way, cols):
        e = in_plane(2, way)
        return remote(
            ysend.at[k, e, :, cols],
            buf.at[par, place_of(k) * NE + yc, :, cols],
            sent.at[4],
            yrs.at[k],
            at_e(e),
            x,
        )

    def near_copy(k, n, cols):
        j = in_plane(*steps[n]) if n < 4 else in_plane(0, 1 - core)
        return remote(
            ysend.at[k, j, :, cols],
            buf.at[par, place_of(k) * NE + yc, :, cols],
            sent.at[4],
            yrs.at[k],
            at_e(j),
            x,
        )

    def forward_copy(k, way):
        src = in_plane(1 if way else -1, core)
        return remote(
            transit.at[k, way],
            buf.at[par, place_of(k) * NE + src],
            sent.at[3],
            yrs.at[k],
            at_e(in_plane(-1 if way else 1, way)),
            x,
        )

    @scoped
    def take(k, part):
        if part == 0:
            arrived(tiles.at[k], irs.at[k])
            if k <= 5:
                tile_copy(k).start()
        cols = pl.ds(part * half, half)
        arrived(zbuf.at[k, :, cols], zrs.at[k, part])
        if k <= 4 or (k, part) in ((5, 1), (6, 0)):
            z_copy(k, part).start()

    @scoped
    def select_block(k):
        place_block(k)
        send_rows(k, slice(0, 2 * half))

    def place_block(k):
        for d in range(1, NE):
            share_copy(k, d).start()
        tile = tiles[k]
        etiles[k, pl.ds(pl.multiple_of(yc * 8, 8), 8)] = tile
        code, gate = codes_of(tile, z * NE, NE)
        pcodes[0, k] = code
        pcodes[1, k] = gate
        want = lax.broadcasted_iota(jnp.int32, (NE, CAP, 128), 1).astype(F32)
        place = (jnp.broadcast_to(code[:, None, :], (NE, CAP, 128)) == want).astype(F32)
        pbuf[k] = place.reshape(NE * CAP, 128).astype(BF16)

    def send_rows(k, cols):
        place = pbuf[k]
        for q in range(cols.start, cols.stop, 512):
            rows = dot(place[:, 0:n_tok], zbuf[k, :, q : q + 512])
            ysend[k, :, :, q : q + 512] = rows.astype(BF16).reshape(NE, CAP, 512)
        for way in range(2):
            (direct_copy if k in DIRECT else transit_copy)(k, way, cols).start()
        for n in (0, 2, 1, 3, 4):
            near_copy(k, n, cols).start()
        buf[par, place_of(k) * NE + yc, :, cols] = ysend[k, yc, :, cols]

    @scoped
    def hand_over(k):
        arrived(transit.at[k], trs.at[k])
        for way in range(2):
            forward_copy(k, way).start()

    half_e = NE // 2

    def x_copy(k, side):
        rows = pl.ds(place_of(k) * NE + side * half_e, half_e)
        return remote(
            buf.at[par, rows],
            buf.at[par, rows],
            sent.at[5],
            xrs.at[k],
            ep,
            left if side else right,
        )

    @scoped
    def x_waits(k):
        arrived(buf.at[1 - par, pl.ds(place_of(k) * NE, NE)], xrs.at[k])

    @scoped
    def y_waits(k):
        arrived(buf.at[par, pl.ds(place_of(k) * NE, NE - 1)], yrs.at[k])

    @scoped
    def pass_on(k):
        y_waits(k)
        x_copy(k, 0).start()
        x_copy(k, 1).start()

    def slot_info(k):
        hit = jnp.zeros((NE, 128), F32)
        gate = jnp.zeros((NE, 128), F32)
        mine = ep.astype(F32)
        for c in range(4):
            here = etiles[k, pl.ds(c, NE, stride=8), :] == mine
            hit = hit + jnp.where(here, 1.0, 0.0)
            gate = gate + jnp.where(here, etiles[k, pl.ds(4 + c, NE, stride=8), :], 0.0)
        return rank_of(hit), gate

    def score_copy(m, d):
        t = (x + d) % 4
        rows = pl.ds(GROUPS[m][0] * NE, GROUPS[m][1] * NE)
        return remote(sx.at[0, rows], sx.at[4 - d, rows], sent.at[6], got.at[0], ep, t)

    def unit(m, which):
        k, n = GROUPS[m]
        return pl.ds(k * NE + which * n * NE // 2, n * NE // 2)

    def halves_copy(m, which, slot):
        peer = near_b if which else near_a
        q = far if slot else peer
        rows = unit(m, which)
        return remote(
            dxq.at[q, rows], r1.at[slot, rows], sent.at[7], r1r.at[m, slot], ep, peer
        )

    def group(m):
        k, n = GROUPS[m]
        return pl.ds(k * NE, n * NE)

    @scoped
    def compute(m):
        first, count = GROUPS[m]
        n_rows = count * NE * CAP
        infos = []
        for n in range(first, first + count):
            share_wait(block_at(n))
            infos.append(slot_info(block_at(n)))
            codes[0, n], codes[1, n] = infos[-1]
        code = jnp.concatenate([i[0] for i in infos], axis=0)
        gate = jnp.concatenate([i[1] for i in infos], axis=0)
        shape = (count * NE, CAP, 128)
        want = lax.broadcasted_iota(jnp.int32, shape, 1).astype(F32)
        mine = jnp.broadcast_to(code[:, None, :], shape) == want
        wide = jnp.where(mine, jnp.broadcast_to(gate[:, None, :], shape), 0.0)
        weight = jnp.sum(wide.reshape(n_rows, 128), axis=1, keepdims=True)
        for n in range(first, first + count):
            x_waits(block_at(n))
        rows = pl.ds(first * NE, count * NE)
        flat = pl.ds(first * NE * CAP, n_rows)
        xin = buf[0, rows].reshape(n_rows, 2048)
        gin = buf[1, rows].reshape(n_rows, 2048)
        gate_pre = dot(xin, wg[...])
        up_pre = dot(xin, wu[...])
        back = dot_last(gin, wd[...])
        glu = jnp.minimum(gate_pre, 7.0)
        lin1 = jnp.clip(up_pre, -7.0, 7.0) + 1.0
        sig = jax.nn.sigmoid(1.702 * glu)
        act = glu * sig
        hidden = lin1 * act
        slope = lin1 * (sig + 1.702 * glu * sig * (1.0 - sig))
        slope = jnp.where(gate_pre < 7.0, slope, 0.0)
        up_slope = jnp.where((up_pre > -7.0) & (up_pre < 7.0), act, 0.0)
        score = jnp.sum(hidden * back, axis=1, keepdims=True)
        d_hidden = weight * back
        d_gate = (d_hidden * slope).astype(BF16)
        d_up = (d_hidden * up_slope).astype(BF16)
        dgu[flat, 0:384] = d_gate
        dgu[flat, 384:768] = d_up
        wtd[flat, :] = (weight * hidden).astype(BF16)
        lane = lax.broadcasted_iota(jnp.int32, shape, 2)
        sub = lax.broadcasted_iota(jnp.int32, shape, 1)
        spread = jnp.broadcast_to(score, (n_rows, 128)).reshape(shape)
        sx[0, rows] = jnp.sum(jnp.where(lane == sub, spread, 0.0), axis=1)
        for d in range(1, 4):
            score_copy(m, d).start()

        for q in range(4):
            cols = slice(512 * q, 512 * (q + 1))
            part = dot_last(d_gate, wg[cols, :]) + dot_last(d_up, wu[cols, :])
            dxq[q, rows] = part.astype(BF16).reshape(count * NE, CAP, 512)
    @scoped
    def send_halves(m):
        for slot in (1, 0):
            for which in range(2):
                halves_copy(m, which, slot).start()

    def quarter_copy(m, which):
        rows = unit(m, which)
        return remote(
            s2.at[rows], r2.at[rows], sent.at[8], r2r.at[m], ep, near_a if which else near_b
        )

    @scoped
    def wait_half(m, slot):
        arrived(r1.at[slot, group(m)], r1r.at[m, slot])

    @scoped
    def wait_quarter(m):
        arrived(r2.at[group(m)], r2r.at[m])

    @scoped
    def reduce_first(m):
        wait_half(m, 1)
        for which in range(2):
            rows = unit(m, which)
            s2[rows] = (
                dxq[near_a if which else near_b, rows].astype(F32) + r1[1, rows].astype(F32)
            ).astype(BF16)
            quarter_copy(m, which).start()
        wait_half(m, 0)
        for which in range(2):
            rows = unit(m, which)
            acc[rows] = dxq[x, rows].astype(F32) + r1[0, rows].astype(F32)

    def back_copy(m, d):
        j = (yc + d) % NE
        ks = pl.ds(*GROUPS[m])
        return remote(yret.at[j, ks], yrr.at[yc, ks], sent.at[9], vrs.at[m], at_e(j), x)

    @scoped
    def reduce_second(m):
        first, count = GROUPS[m]
        wait_quarter(m)
        for k in range(first, first + count):
            rows = pl.ds(k * NE, NE)
            total = (acc[rows] + r2[rows].astype(F32)).astype(BF16)
            for j in range(NE):
                yret[j, k] = total[j]
        for d in (1, 7, 2, 6, 3, 5, 4):
            back_copy(m, d).start()
        ks = pl.ds(first, count)
        yrr[yc, ks] = yret[yc, ks]

    def home_copy(k):
        return remote(
            wsend.at[k], wrecv.at[PAIR_OF[k]], sent.at[10], got.at[1], at_z(z_of(k)), x
        )

    @scoped
    def back_waits(m):
        arrived(yrr.at[pl.ds(0, NE - 1), pl.ds(*GROUPS[m])], vrs.at[m])

    @scoped
    def combine(m):
        back_waits(m)
        first, count = GROUPS[m]
        for n in range(first, first + count):
            k = block_at(n)
            rows = jnp.concatenate([yrr[j, n] for j in range(NE)], axis=0)
            wsend[k] = dot_first(pbuf[k][:, 0:n_tok], rows).astype(BF16)
            if k > 0:
                home_copy(k).start()

    def both(f, *ks):
        for k in ks:
            f(k)

    def takes(part, *ks):
        for k in ks:
            take(k, part)

    first_half, second_half = slice(0, half), slice(half, 2 * half)
    select_block(0)
    hand_over(0)
    takes(0, 1, 2)
    place_block(1)
    send_rows(1, first_half)
    place_block(2)
    send_rows(2, first_half)
    takes(1, 1, 2)
    send_rows(1, second_half)
    send_rows(2, second_half)
    takes(0, 3, 4)
    pass_on(0)
    takes(1, 3, 4)
    select_block(3)
    pass_on(1)
    select_block(4)
    pass_on(2)
    hand_over(3)
    takes(0, 5, 6)
    hand_over(4)
    takes(1, 5, 6)
    select_block(5)
    pass_on(3)
    select_block(6)
    take(7, 0)
    take(7, 1)
    hand_over(5)
    select_block(7)
    pass_on(4)
    hand_over(6)
    load_g.wait()
    load_u.wait()
    load_d.wait()
    compute(0)
    pass_on(5)
    hand_over(7)
    pass_on(6)
    pass_on(7)
    compute(1)
    send_halves(1)
    compute(2)
    send_halves(2)
    compute(3)
    send_halves(3)
    reduce_first(1)

    @scoped
    def weight_tile(i, carry):
        cols = pl.ds(pl.multiple_of(i * 256, 256), 256)
        xs = buf[0, :, :, cols].reshape(512, 256)
        both = dot_first(xs, dgu[...]).astype(BF16)
        gg_ref[cols, :] = both[:, 0:384]
        ug_ref[cols, :] = both[:, 384:768]
        gs = buf[1, :, :, cols].reshape(512, 256)
        dg_ref[:, cols] = dot_first(wtd[...], gs).astype(BF16)
        return carry

    def weight_tiles(a, b):
        lax.fori_loop(a, b, weight_tile, 0)

    def sy_copy(d):
        j = (yc + d) % NE
        return remote(sy.at[j], syr.at[yc], sent.at[11], got.at[2], at_e(j), x)

    @scoped
    def scores_x():
        arrived(sx.at[pl.ds(1, 3)], got.at[0])
        sx[1] = (sx[0] + sx[1]) + (sx[2] + sx[3])
        for j in range(NE):
            sy[j] = jnp.concatenate(
                [sx[1, k * NE + j : k * NE + j + 1, :] for k in range(NK)], axis=0
            )
        for d in range(1, NE):
            sy_copy(d).start()
        syr[yc] = sy[yc]

    def sz_copy(k):
        return remote(
            szs.at[place_of(k)],
            smat.at[pl.ds(pl.multiple_of(z * NE, NE), NE)],
            sent.at[12],
            got.at[3],
            at_z(z_of(k)),
            x,
        )

    def mean_copy(k):
        return remote(
            means.at[0],
            means.at[PAIR_OF[k]],
            sent.at[13],
            got.at[4],
            at_z(z_of(k)),
            x,
        )

    def at_ranks(code, scores):
        found = jnp.zeros(code.shape, F32)
        for r in range(CAP):
            found = found + jnp.where(code == float(r), scores[:, r : r + 1], 0.0)
        return found

    @scoped
    def scores_y():
        arrived(syr.at[pl.ds(0, NE - 1)], got.at[2])
        for n in range(NK):
            k = block_at(n)
            szs[n] = jnp.concatenate([syr[e, n : n + 1, :] for e in range(NE)], axis=0)
            part = pcodes[1, k] * at_ranks(pcodes[0, k], szs[n])
            means[0, pl.ds(z_of(k), 1), :] = jnp.sum(part, axis=0, keepdims=True)
        for k in range(1, NK):
            mean_copy(k).start()
        for k in range(1, NK):
            sz_copy(k).start()
        smat[pl.ds(pl.multiple_of(z * NE, NE), NE), :] = szs[place_of(0)]

    def dy_copy(d):
        j = (yc + d) % NE
        return remote(dys, de.at[yc], sent.at[14], got.at[5], at_e(j), x)

    @scoped
    def scores_z():
        arrived(means.at[pl.ds(1, NK - 1)], got.at[4])
        total = means[0]
        for k in range(1, NK):
            total = total + means[k]
        dys[...] = total
        for d in range(1, NE):
            dy_copy(d).start()
        de[yc] = total

    @scoped
    def home_logits():
        arrived(smat.at[pl.ds(0, NE * (NK - 1))], got.at[3])
        code_t, gate_t = codes_of(tiles[0], 0, n_exp)
        score_at = at_ranks(code_t, smat)
        mean = jnp.sum(gate_t * score_at, axis=0, keepdims=True)
        dmat[...] = jnp.where(code_t >= 0.0, gate_t * (score_at - mean), 0.0)

    x_rows = pl.ds(pl.multiple_of(x * 512, 512), 512)

    @scoped
    def token_out():
        d_t = dmat[...]
        d_hi = d_t.astype(BF16)
        d_lo = (d_t - d_hi.astype(F32)).astype(BF16)
        rw_x = rwv[:, x_rows]
        total = (dot_first(d_hi, rw_x) + dot_first(d_lo, rw_x))[0:n_tok, :]
        total = total + wsend[0].astype(F32)
        arrived(wrecv.at[pl.ds(1, NK - 1)], got.at[1])
        for k in range(1, NK):
            total = total + wrecv[k].astype(F32)
        tg_ref[...] = total.astype(BF16)

    @scoped
    def router_out():
        arrived(de.at[pl.ds(0, NE - 1)], got.at[5])
        shape = (NE, CAP, 128)
        want = lax.broadcasted_iota(jnp.int32, shape, 1).astype(F32)
        lane = lax.broadcasted_iota(jnp.int32, shape, 2)
        sub = lax.broadcasted_iota(jnp.int32, shape, 1)
        sums = jnp.zeros((CAP, 512), F32)

        def of_slots(mask, rows):
            wide = jnp.where(mask, jnp.broadcast_to(rows[:, None, :], shape), 0.0)
            return jnp.sum(wide, axis=2, keepdims=True)

        for n in range(NK):
            mean = jnp.concatenate([de[j, pl.ds(z_of(block_at(n)), 1), :] for j in range(NE)], axis=0)
            code, gate = codes[0, n], codes[1, n]
            mine = jnp.broadcast_to(code[:, None, :], shape) == want
            score = of_slots(lane == sub, sx[1, n * NE : (n + 1) * NE, :])
            slot_d = of_slots(mine, gate) * (score - of_slots(mine, mean))
            rows = buf[0, n * NE : (n + 1) * NE, :, x_rows].astype(F32)
            sums = sums + jnp.sum(slot_d * rows, axis=0)
        rg_ref[...] = jnp.sum(sums, axis=0, keepdims=True)

    weight_tiles(0, 2)
    reduce_first(2)
    send_halves(0)
    scores_x()
    reduce_first(3)
    reduce_second(1)
    weight_tiles(2, 3)
    reduce_second(2)
    scores_y()
    combine(1)
    weight_tiles(3, 4)
    reduce_first(0)
    reduce_second(3)
    combine(2)
    weight_tiles(4, 6)
    reduce_second(0)
    scores_z()
    combine(3)
    weight_tiles(6, 8)
    combine(0)
    home_logits()
    router_out()
    token_out()

    with jax.named_scope("drain_all"):
        seven = pl.ds(0, 7)
        for i, ref in enumerate(
            (
                zbuf.at[seven],
                tiles.at[seven],
                etiles.at[seven, pl.ds(0, 64)],
                buf.at[0, pl.ds(0, 4 * (NK - len(DIRECT)))],
                buf.at[0, pl.ds(0, 5 * NK + 2 * len(DIRECT))],
                buf.at[0],
                sx.at[pl.ds(0, 3)],
                r1,
                s2,
                yret.at[seven],
                wsend.at[seven],
                sy.at[seven],
                szs.at[seven],
                means.at[seven],
                means.at[seven],
            )
        ):
            arrived(ref, sent.at[i])


def finish_kernel(tg, rg, gg, ug, dg, tg_o, rg_o, gg_o, ug_o, dg_o, sems):
    pairs = ((gg, gg_o), (ug, ug_o), (dg, dg_o), (tg, tg_o), (rg, rg_o))
    copies = [pltpu.make_async_copy(a, b, sems.at[i]) for i, (a, b) in enumerate(pairs)]
    for c in copies:
        c.start()
    for c in copies:
        c.wait()


def per_device(tokens, out_grad, expert_ids, router_weight, w_gate, w_up, w_down):
    n_tok, width = tokens.shape
    n_exp = router_weight.shape[1]
    top_count = expert_ids.shape[1]
    ff = w_gate.shape[2]
    quarter = width // 4
    any_space = pl.BlockSpec(memory_space=pl.ANY)
    vmem = pl.BlockSpec(memory_space=pltpu.VMEM)
    hbm = pl.BlockSpec(memory_space=pltpu.HBM)
    dma = pltpu.SemaphoreType.DMA
    slots = NK * NE
    scratch = [
        pltpu.VMEM((n_tok, width), BF16),
        pltpu.VMEM((top_count, n_tok), jnp.int32),
        pltpu.VMEM((n_exp, width), BF16),
        pltpu.VMEM((width, ff), BF16),
        pltpu.VMEM((width, ff), BF16),
        pltpu.VMEM((ff, width), BF16),
        pltpu.VMEM((NK, n_tok, width), BF16),
        pltpu.VMEM((NK, 8, 128), F32),
        pltpu.VMEM((NK, NE * 8, 128), F32),
        pltpu.VMEM((2, NK, NE, 128), F32),
        pltpu.VMEM((2, NK, NE, 128), F32),
        pltpu.VMEM((128, 128), BF16),
        pltpu.VMEM((NK, 2, CAP, width), BF16),
        pltpu.VMEM((NK, NE * CAP, 128), BF16),
        pltpu.VMEM((NK, NE, CAP, width), BF16),
        pltpu.VMEM((2, slots, CAP, width), BF16),
        pltpu.VMEM((slots * CAP, 2 * ff), BF16),
        pltpu.VMEM((slots * CAP, ff), BF16),
        pltpu.VMEM((4, slots, CAP, quarter), BF16),
        pltpu.VMEM((2, slots, CAP, quarter), BF16),
        pltpu.VMEM((slots, CAP, quarter), F32),
        pltpu.VMEM((slots, CAP, quarter), BF16),
        pltpu.VMEM((slots, CAP, quarter), BF16),
        pltpu.VMEM((NE, NK, CAP, quarter), BF16),
        pltpu.VMEM((NE, NK, CAP, quarter), BF16),
        pltpu.VMEM((NK, n_tok, quarter), BF16),
        pltpu.VMEM((NK, n_tok, quarter), BF16),
        pltpu.VMEM((4, slots, 128), F32),
        pltpu.VMEM((NE, NK, 128), F32),
        pltpu.VMEM((NE, NK, 128), F32),
        pltpu.VMEM((NK, NE, 128), F32),
        pltpu.VMEM((n_exp, 128), F32),
        pltpu.VMEM((n_exp, 128), F32),
        pltpu.VMEM((NK, NK, 128), F32),
        pltpu.VMEM((NK, 128), F32),
        pltpu.VMEM((NE, NK, 128), F32),
        dma((7,)),
        dma((15,)),
        dma((6,)),
        dma((8, 2)),
        dma((8,)),
        dma((8,)),
        dma((8,)),
        dma((8,)),
        dma((8,)),
        dma((4, 2)),
        dma((4,)),
        dma((4,)),
    ]
    shapes = (
        jax.ShapeDtypeStruct((n_tok, quarter), BF16),
        jax.ShapeDtypeStruct((1, quarter), F32),
        jax.ShapeDtypeStruct((width, ff), BF16),
        jax.ShapeDtypeStruct((width, ff), BF16),
        jax.ShapeDtypeStruct((ff, width), BF16),
    )
    out = pl.pallas_call(
        step_kernel,
        name="moe_backward",
        out_shape=shapes,
        in_specs=[hbm] * 7,
        out_specs=(vmem,) * 5,
        scratch_shapes=scratch,
        compiler_params=pltpu.CompilerParams(
            collective_id=0, has_side_effects=True, vmem_limit_bytes=40 * 1024 * 1024
        ),
    )(
        *(
            pltpu.with_memory_space_constraint(a, pltpu.HBM)
            for a in (
                tokens,
                out_grad,
                expert_ids.T,
                router_weight.T,
                w_gate[0],
                w_up[0],
                w_down[0],
            )
        )
    )
    token_grad, router_grad, gate_grad, up_grad, down_grad = pl.pallas_call(
        finish_kernel,
        name="finish",
        out_shape=shapes,
        in_specs=[any_space] * 5,
        out_specs=(any_space,) * 5,
        scratch_shapes=[dma((5,))],
        compiler_params=pltpu.CompilerParams(vmem_limit_bytes=4 * 1024 * 1024),
    )(*out)
    return (
        token_grad,
        router_grad.reshape(quarter, 1),
        gate_grad[None],
        up_grad[None],
        down_grad[None],
    )


def solution(mesh):
    in_specs = (
        P("ep", None),
        P("ep", None),
        P("ep", None),
        P(),
        P("ep", None, "tp"),
        P("ep", None, "tp"),
        P("ep", "tp", None),
    )
    out_specs = (
        P("ep", "tp"),
        P("tp", "ep"),
        P("ep", None, "tp"),
        P("ep", None, "tp"),
        P("ep", "tp", None),
    )
    return jax.shard_map(
        per_device, mesh=mesh, in_specs=in_specs, out_specs=out_specs, check_vma=False
    )
```

```python
import functools

import jax
import jax.numpy as jnp
from jax import lax
from jax.experimental import pallas as pl
from jax.experimental.pallas import tpu as pltpu
from jax.sharding import PartitionSpec as P

MESH = pl.DeviceIdType.MESH
F32 = jnp.float32
BF16 = jnp.bfloat16
NK = 8
NE = 8
CAP = 8
PAIR_OF = (0, 2, 1, 4, 3, 6, 5, 7)
GROUPS = ((0, 2), (2, 2), (4, 2), (6, 2))
SUMMED = (None, (2, 2), (4, 2), (6, 1))
WIDE = (1, 2, 0)
DIRECT = (1, 2)


def place_of(k):
    return (k + NK - 1) % NK


def block_at(n):
    return (n + 1) % NK


def scoped(f):
    @functools.wraps(f)
    def run(*args):
        with jax.named_scope(f.__name__):
            return f(*args)

    return run


def dot_last(a, b):
    return lax.dot_general(a, b, (((1,), (1,)), ((), ())), preferred_element_type=F32)


def dot_first(a, b):
    return lax.dot_general(a, b, (((0,), (0,)), ((), ())), preferred_element_type=F32)


def dot(a, b):
    return jnp.dot(a, b, preferred_element_type=F32)


def step_kernel(
    tok_hbm,
    grad_hbm,
    ids_hbm,
    rw_hbm,
    wg_hbm,
    wu_hbm,
    wd_hbm,
    tg_ref,
    rg_ref,
    gg_ref,
    ug_ref,
    dg_ref,
    tokv,
    idsv,
    rwv,
    wg,
    wu,
    wd,
    zbuf,
    tiles,
    etiles,
    codes,
    pcodes,
    upper,
    transit,
    pbuf,
    ysend,
    buf,
    dgu,
    wtd,
    dxq,
    r1,
    acc,
    s2,
    r2,
    yret,
    yrr,
    wide,
    hzs,
    hzr,
    hxs,
    hxr,
    wsend,
    wrecv,
    sx,
    sy,
    syr,
    szs,
    smat,
    dmat,
    means,
    dys,
    de,
    ld,
    sent,
    got,
    zrs,
    irs,
    ers,
    trs,
    yrs,
    xrs,
    r1r,
    r2r,
    vrs,
    wyr,
):
    ep = lax.axis_index("ep")
    x = lax.axis_index("tp")
    z = ep // NE
    yc = ep % NE
    y = yc // 2
    core = yc % 2
    par = x % 2
    odd = x % 2
    near_a = x + 1 - 2 * odd
    near_b = (x + 3 + 2 * odd) % 4
    far = (x + 2) % 4
    right = (x + 1) % 4
    left = (x + 3) % 4

    def remote(src, dst, ss, rs, e, t):
        return pltpu.make_async_remote_copy(
            src_ref=src,
            dst_ref=dst,
            send_sem=ss,
            recv_sem=rs,
            device_id={"ep": e, "tp": t},
            device_id_type=MESH,
        )

    def arrived(ref, sem):
        pltpu.make_async_copy(ref, ref, sem).wait()

    def z_of(k):
        h = (k + 1) // 2
        s = 1 - 2 * ((k + 1) % 2)
        return (z + s * h + NK) % NK

    def at_z(zz):
        return zz * NE + yc

    def at_e(j):
        return z * NE + j

    def in_plane(dy, c):
        return ((y + dy + 4) % 4) * 2 + c

    barrier = pltpu.get_barrier_semaphore()
    for d in (1, NK - 1):
        pl.semaphore_signal(
            barrier, inc=1, device_id={"ep": at_z((z + d) % NK), "tp": x}, device_id_type=MESH
        )
    for d in range(1, NE):
        pl.semaphore_signal(
            barrier, inc=1, device_id={"ep": at_e((yc + d) % NE), "tp": x}, device_id_type=MESH
        )
    for d in range(1, 4):
        pl.semaphore_signal(
            barrier, inc=1, device_id={"ep": ep, "tp": (x + d) % 4}, device_id_type=MESH
        )

    load_tok = pltpu.make_async_copy(tok_hbm, tokv, ld.at[0])
    load_tok.start()
    load_ids = pltpu.make_async_copy(ids_hbm, idsv, ld.at[5])
    load_rw = pltpu.make_async_copy(rw_hbm, rwv, ld.at[6])
    load_ids.start()
    load_rw.start()

    @pl.when(par == 0)
    def _():
        pltpu.make_async_copy(tok_hbm, zbuf.at[0], ld.at[1]).start()

    @pl.when(par == 1)
    def _():
        pltpu.make_async_copy(grad_hbm, zbuf.at[0], ld.at[1]).start()

    load_g = pltpu.make_async_copy(wg_hbm, wg, ld.at[2])
    load_u = pltpu.make_async_copy(wu_hbm, wu, ld.at[3])
    load_d = pltpu.make_async_copy(wd_hbm, wd, ld.at[4])
    load_g.start()
    load_u.start()
    load_d.start()

    @scoped
    def wait_small():
        load_tok.wait()
        load_ids.wait()
        load_rw.wait()

    @scoped
    def wait_barrier():
        pl.semaphore_wait(barrier, 2 + (NE - 1) + 3)

    wait_barrier()

    pltpu.make_async_copy(tok_hbm, zbuf.at[0], ld.at[1]).wait()

    half = zbuf.shape[2] // 2

    def z_copy(k, part):
        to = 7 if k >= 5 else k + 2
        s = 1 - 2 * ((k + 1) % 2)
        cols = pl.ds(part * half, half)
        return remote(
            zbuf.at[k, :, cols],
            zbuf.at[to, :, cols],
            sent.at[0],
            zrs.at[to, part],
            at_z((z - s + NK) % NK),
            x,
        )

    def z_first(part, way):
        cols = pl.ds(part * half, half)
        return remote(
            zbuf.at[0, :, cols],
            zbuf.at[1 + way, :, cols],
            sent.at[0],
            zrs.at[1 + way, part],
            at_z((z + 1) % NK) if way else at_z((z + NK - 1) % NK),
            x,
        )

    def tile_copy(k):
        s = 1 - 2 * ((k + 1) % 2)
        return remote(
            tiles.at[k], tiles.at[k + 2], sent.at[1], irs.at[k + 2], at_z((z - s + NK) % NK), x
        )

    below, above = at_z((z + NK - 1) % NK), at_z((z + 1) % NK)
    t_left = remote(tiles.at[0], tiles.at[1], sent.at[1], irs.at[1], below, x)
    t_right = remote(tiles.at[0], tiles.at[2], sent.at[1], irs.at[2], above, x)
    z_first(0, 0).start()
    z_first(0, 1).start()
    wait_small()
    n_tok = tokv.shape[0]
    n_exp = rwv.shape[0]
    logits = dot_last(rwv[...], tokv[...])
    expert = lax.broadcasted_iota(jnp.int32, (n_exp, n_tok), 0)
    picked = []
    for k in range(idsv.shape[0]):
        here = idsv[k : k + 1, :] == expert
        picked.append(jnp.sum(jnp.where(here, logits, 0.0), axis=0, keepdims=True))
    picked = jnp.concatenate(picked, axis=0)
    expd = jnp.exp(picked - jnp.max(picked, axis=0, keepdims=True))
    gates = expd / jnp.sum(expd, axis=0, keepdims=True)
    tiles[0] = jnp.full((8, 128), -1.0, F32)
    tiles[0, 0:4, 0:n_tok] = idsv[...].astype(F32)
    tiles[0, 4:8, 0:n_tok] = gates
    row = lax.broadcasted_iota(jnp.int32, (128, 128), 0)
    col = lax.broadcasted_iota(jnp.int32, (128, 128), 1)
    upper[...] = jnp.where(row < col, 1.0, 0.0).astype(BF16)

    def rank_of(hit):
        return jnp.where(hit > 0.0, dot(hit.astype(BF16), upper[...]), -1.0)

    def codes_of(tile, first, count):
        experts = (lax.broadcasted_iota(jnp.int32, (count, 128), 0) + first).astype(F32)
        hit = jnp.zeros((count, 128), F32)
        gate = jnp.zeros((count, 128), F32)
        for k in range(4):
            here = tile[k : k + 1, :] == experts
            hit = hit + jnp.where(here, 1.0, 0.0)
            gate = gate + jnp.where(here, tile[4 + k : 5 + k, :], 0.0)
        return rank_of(hit), gate

    t_left.start()
    t_right.start()
    z_first(1, 0).start()
    z_first(1, 1).start()

    def share_copy(k, d):
        j = (yc + d) % NE
        return remote(
            tiles.at[k],
            etiles.at[k, pl.ds(pl.multiple_of(yc * 8, 8), 8)],
            sent.at[2],
            ers.at[k],
            at_e(j),
            x,
        )

    def share_wait(k):
        arrived(etiles.at[k, pl.ds(0, 8 * (NE - 1))], ers.at[k])

    steps = ((1, 0), (1, 1), (-1, 0), (-1, 1))

    def transit_copy(k, way, cols):
        e = in_plane(2, way)
        return remote(
            ysend.at[k, e],
            transit.at[k, way],
            sent.at[3],
            trs.at[k],
            at_e(in_plane(-1 if way else 1, core)),
            x,
        )

    def direct_copy(k, way, cols):
        e = in_plane(2, way)
        return remote(
            ysend.at[k, e, :, cols],
            buf.at[par, place_of(k) * NE + yc, :, cols],
            sent.at[4],
            yrs.at[k],
            at_e(e),
            x,
        )

    def near_copy(k, n, cols):
        j = in_plane(*steps[n]) if n < 4 else in_plane(0, 1 - core)
        return remote(
            ysend.at[k, j, :, cols],
            buf.at[par, place_of(k) * NE + yc, :, cols],
            sent.at[4],
            yrs.at[k],
            at_e(j),
            x,
        )

    def forward_copy(k, way):
        src = in_plane(1 if way else -1, core)
        return remote(
            transit.at[k, way],
            buf.at[par, place_of(k) * NE + src],
            sent.at[3],
            yrs.at[k],
            at_e(in_plane(-1 if way else 1, way)),
            x,
        )

    @scoped
    def take(k, part):
        if part == 0:
            arrived(tiles.at[k], irs.at[k])
            if k <= 5:
                tile_copy(k).start()
        cols = pl.ds(part * half, half)
        arrived(zbuf.at[k, :, cols], zrs.at[k, part])
        if k <= 4 or (k, part) in ((5, 1), (6, 0)):
            z_copy(k, part).start()

    @scoped
    def select_block(k):
        place_block(k)
        send_rows(k, slice(0, 2 * half))

    def place_block(k):
        for d in range(1, NE):
            share_copy(k, d).start()
        tile = tiles[k]
        etiles[k, pl.ds(pl.multiple_of(yc * 8, 8), 8)] = tile
        code, gate = codes_of(tile, z * NE, NE)
        pcodes[0, k] = code
        pcodes[1, k] = gate
        want = lax.broadcasted_iota(jnp.int32, (NE, CAP, 128), 1).astype(F32)
        place = (jnp.broadcast_to(code[:, None, :], (NE, CAP, 128)) == want).astype(F32)
        pbuf[k] = place.reshape(NE * CAP, 128).astype(BF16)

    def send_rows(k, cols):
        place = pbuf[k]
        for q in range(cols.start, cols.stop, 512):
            rows = dot(place[:, 0:n_tok], zbuf[k, :, q : q + 512])
            ysend[k, :, :, q : q + 512] = rows.astype(BF16).reshape(NE, CAP, 512)
        for way in range(2):
            (direct_copy if k in DIRECT else transit_copy)(k, way, cols).start()
        for n in (0, 2, 1, 3, 4):
            near_copy(k, n, cols).start()
        buf[par, place_of(k) * NE + yc, :, cols] = ysend[k, yc, :, cols]

    @scoped
    def hand_over(k):
        arrived(transit.at[k], trs.at[k])
        for way in range(2):
            forward_copy(k, way).start()

    half_e = NE // 2

    def x_copy(k, side):
        rows = pl.ds(place_of(k) * NE + side * half_e, half_e)
        return remote(
            buf.at[par, rows],
            buf.at[par, rows],
            sent.at[5],
            xrs.at[k],
            ep,
            left if side else right,
        )

    @scoped
    def x_waits(k):
        arrived(buf.at[1 - par, pl.ds(place_of(k) * NE, NE)], xrs.at[k])

    @scoped
    def y_waits(k):
        arrived(buf.at[par, pl.ds(place_of(k) * NE, NE - 1)], yrs.at[k])

    @scoped
    def pass_on(k):
        y_waits(k)
        x_copy(k, 0).start()
        x_copy(k, 1).start()

    def slot_info(k):
        hit = jnp.zeros((NE, 128), F32)
        gate = jnp.zeros((NE, 128), F32)
        mine = ep.astype(F32)
        for c in range(4):
            here = etiles[k, pl.ds(c, NE, stride=8), :] == mine
            hit = hit + jnp.where(here, 1.0, 0.0)
            gate = gate + jnp.where(here, etiles[k, pl.ds(4 + c, NE, stride=8), :], 0.0)
        return rank_of(hit), gate

    def score_copy(m, d):
        t = (x + d) % 4
        rows = pl.ds(GROUPS[m][0] * NE, GROUPS[m][1] * NE)
        return remote(sx.at[0, rows], sx.at[4 - d, rows], sent.at[6], got.at[0], ep, t)

    def unit(m, which):
        n, count = SUMMED[m]
        return pl.ds(n * NE + which * count * NE // 2, count * NE // 2)

    def halves_copy(m, which, slot):
        peer = near_b if which else near_a
        q = far if slot else peer
        rows = unit(m, which)
        return remote(
            dxq.at[q, rows], r1.at[slot, rows], sent.at[7], r1r.at[m, slot], ep, peer
        )

    def group(m):
        n, count = SUMMED[m]
        return pl.ds(n * NE, count * NE)

    @scoped
    def compute(m):
        first, count = GROUPS[m]
        n_rows = count * NE * CAP
        infos = []
        for n in range(first, first + count):
            share_wait(block_at(n))
            infos.append(slot_info(block_at(n)))
            codes[0, n], codes[1, n] = infos[-1]
        code = jnp.concatenate([i[0] for i in infos], axis=0)
        gate = jnp.concatenate([i[1] for i in infos], axis=0)
        shape = (count * NE, CAP, 128)
        want = lax.broadcasted_iota(jnp.int32, shape, 1).astype(F32)
        mine = jnp.broadcast_to(code[:, None, :], shape) == want
        wide = jnp.where(mine, jnp.broadcast_to(gate[:, None, :], shape), 0.0)
        weight = jnp.sum(wide.reshape(n_rows, 128), axis=1, keepdims=True)
        for n in range(first, first + count):
            x_waits(block_at(n))
        rows = pl.ds(first * NE, count * NE)
        flat = pl.ds(first * NE * CAP, n_rows)
        xin = buf[0, rows].reshape(n_rows, 2048)
        gin = buf[1, rows].reshape(n_rows, 2048)
        gate_pre = dot(xin, wg[...])
        up_pre = dot(xin, wu[...])
        back = dot_last(gin, wd[...])
        glu = jnp.minimum(gate_pre, 7.0)
        lin1 = jnp.clip(up_pre, -7.0, 7.0) + 1.0
        sig = jax.nn.sigmoid(1.702 * glu)
        act = glu * sig
        hidden = lin1 * act
        slope = lin1 * (sig + 1.702 * glu * sig * (1.0 - sig))
        slope = jnp.where(gate_pre < 7.0, slope, 0.0)
        up_slope = jnp.where((up_pre > -7.0) & (up_pre < 7.0), act, 0.0)
        score = jnp.sum(hidden * back, axis=1, keepdims=True)
        d_hidden = weight * back
        d_gate = (d_hidden * slope).astype(BF16)
        d_up = (d_hidden * up_slope).astype(BF16)
        dgu[flat, 0:384] = d_gate
        dgu[flat, 384:768] = d_up
        wtd[flat, :] = (weight * hidden).astype(BF16)
        lane = lax.broadcasted_iota(jnp.int32, shape, 2)
        sub = lax.broadcasted_iota(jnp.int32, shape, 1)
        spread = jnp.broadcast_to(score, (n_rows, 128)).reshape(shape)
        sx[0, rows] = jnp.sum(jnp.where(lane == sub, spread, 0.0), axis=1)
        for d in range(1, 4):
            score_copy(m, d).start()

        for q in range(4):
            cols = slice(512 * q, 512 * (q + 1))
            part = dot_last(d_gate, wg[cols, :]) + dot_last(d_up, wu[cols, :])
            dxq[q, rows] = part.astype(BF16).reshape(count * NE, CAP, 512)
    @scoped
    def send_halves(m):
        for slot in (1, 0):
            for which in range(2):
                halves_copy(m, which, slot).start()

    def quarter_copy(m, which):
        rows = unit(m, which)
        return remote(
            s2.at[rows], r2.at[rows], sent.at[8], r2r.at[m], ep, near_a if which else near_b
        )

    @scoped
    def wait_half(m, slot):
        arrived(r1.at[slot, group(m)], r1r.at[m, slot])

    @scoped
    def wait_quarter(m):
        arrived(r2.at[group(m)], r2r.at[m])

    @scoped
    def reduce_first(m):
        wait_half(m, 1)
        for which in range(2):
            rows = unit(m, which)
            s2[rows] = (
                dxq[near_a if which else near_b, rows].astype(F32) + r1[1, rows].astype(F32)
            ).astype(BF16)
            quarter_copy(m, which).start()
        wait_half(m, 0)
        for which in range(2):
            rows = unit(m, which)
            acc[rows] = dxq[x, rows].astype(F32) + r1[0, rows].astype(F32)

    def back_copy(m, d):
        j = (yc + d) % NE
        ks = pl.ds(*SUMMED[m])
        return remote(yret.at[j, ks], yrr.at[yc, ks], sent.at[9], vrs.at[m], at_e(j), x)

    @scoped
    def reduce_second(m):
        first, count = SUMMED[m]
        wait_quarter(m)
        for k in range(first, first + count):
            rows = pl.ds(k * NE, NE)
            total = (acc[rows] + r2[rows].astype(F32)).astype(BF16)
            for j in range(NE):
                yret[j, k] = total[j]
        for d in (1, 7, 2, 6, 3, 5, 4):
            back_copy(m, d).start()
        ks = pl.ds(first, count)
        yrr[yc, ks] = yret[yc, ks]

    def home_copy(k):
        return remote(
            wsend.at[k], wrecv.at[PAIR_OF[k]], sent.at[10], got.at[1], at_z(z_of(k)), x
        )

    @scoped
    def back_waits(m):
        arrived(yrr.at[pl.ds(0, NE - 1), pl.ds(*SUMMED[m])], vrs.at[m])

    @scoped
    def combine(m):
        back_waits(m)
        first, count = SUMMED[m]
        for n in range(first, first + count):
            k = block_at(n)
            rows = jnp.concatenate([yrr[j, n] for j in range(NE)], axis=0)
            wsend[k] = dot_first(pbuf[k][:, 0:n_tok], rows).astype(BF16)
            home_copy(k).start()

    @scoped
    def wide_send(w):
        n = place_of(WIDE[w])
        for d in (1, 7, 2, 6, 3, 5, 4):
            j = (yc + d) % NE
            remote(
                dxq.at[:, n * NE + j], wide.at[w, yc], sent.at[15], wyr.at[w], at_e(j), x
            ).start()
        wide[w, yc] = dxq[:, n * NE + yc]

    @scoped
    def wide_combine(w):
        arrived(wide.at[w, pl.ds(0, NE - 1)], wyr.at[w])
        k = WIDE[w]
        place = pbuf[k][:, 0:n_tok]
        for q in range(4):
            rows = jnp.concatenate([wide[w, j, q] for j in range(NE)], axis=0)
            hzs[w, q] = dot_first(place, rows).astype(BF16)
        if k:
            remote(
                hzs.at[w], hzr.at[PAIR_OF[k] - 1], sent.at[16], got.at[6], at_z(z_of(k)), x
            ).start()

    @scoped
    def wide_home():
        arrived(hzr, got.at[6])
        hxs[...] = (
            hzs[2].astype(F32) + hzr[0].astype(F32) + hzr[1].astype(F32)
        ).astype(BF16)
        for d in (1, 3, 2):
            t = (x + d) % 4
            remote(hxs.at[t], hxr.at[3 - d], sent.at[17], got.at[7], ep, t).start()

    def both(f, *ks):
        for k in ks:
            f(k)

    def takes(part, *ks):
        for k in ks:
            take(k, part)

    first_half, second_half = slice(0, half), slice(half, 2 * half)
    select_block(0)
    hand_over(0)
    takes(0, 1, 2)
    place_block(1)
    send_rows(1, first_half)
    place_block(2)
    send_rows(2, first_half)
    takes(1, 1, 2)
    send_rows(1, second_half)
    send_rows(2, second_half)
    takes(0, 3, 4)
    pass_on(0)
    takes(1, 3, 4)
    select_block(3)
    pass_on(1)
    select_block(4)
    pass_on(2)
    hand_over(3)
    takes(0, 5, 6)
    hand_over(4)
    takes(1, 5, 6)
    select_block(5)
    pass_on(3)
    select_block(6)
    take(7, 0)
    take(7, 1)
    hand_over(5)
    select_block(7)
    pass_on(4)
    hand_over(6)
    load_g.wait()
    load_u.wait()
    load_d.wait()
    compute(0)
    pass_on(5)
    hand_over(7)
    wide_send(0)
    wide_send(1)
    pass_on(6)
    pass_on(7)
    compute(1)
    send_halves(1)
    compute(2)
    send_halves(2)
    compute(3)
    send_halves(3)
    wide_send(2)
    reduce_first(1)

    @scoped
    def weight_tile(i, carry):
        cols = pl.ds(pl.multiple_of(i * 256, 256), 256)
        xs = buf[0, :, :, cols].reshape(512, 256)
        both = dot_first(xs, dgu[...]).astype(BF16)
        gg_ref[cols, :] = both[:, 0:384]
        ug_ref[cols, :] = both[:, 384:768]
        gs = buf[1, :, :, cols].reshape(512, 256)
        dg_ref[:, cols] = dot_first(wtd[...], gs).astype(BF16)
        return carry

    def weight_tiles(a, b):
        lax.fori_loop(a, b, weight_tile, 0)

    def sy_copy(d):
        j = (yc + d) % NE
        return remote(sy.at[j], syr.at[yc], sent.at[11], got.at[2], at_e(j), x)

    @scoped
    def scores_x():
        arrived(sx.at[pl.ds(1, 3)], got.at[0])
        sx[1] = (sx[0] + sx[1]) + (sx[2] + sx[3])
        for j in range(NE):
            sy[j] = jnp.concatenate(
                [sx[1, k * NE + j : k * NE + j + 1, :] for k in range(NK)], axis=0
            )
        for d in range(1, NE):
            sy_copy(d).start()
        syr[yc] = sy[yc]

    def sz_copy(k):
        return remote(
            szs.at[place_of(k)],
            smat.at[pl.ds(pl.multiple_of(z * NE, NE), NE)],
            sent.at[12],
            got.at[3],
            at_z(z_of(k)),
            x,
        )

    def mean_copy(k):
        return remote(
            means.at[0],
            means.at[PAIR_OF[k]],
            sent.at[13],
            got.at[4],
            at_z(z_of(k)),
            x,
        )

    def at_ranks(code, scores):
        found = jnp.zeros(code.shape, F32)
        for r in range(CAP):
            found = found + jnp.where(code == float(r), scores[:, r : r + 1], 0.0)
        return found

    @scoped
    def scores_y():
        arrived(syr.at[pl.ds(0, NE - 1)], got.at[2])
        for n in range(NK):
            k = block_at(n)
            szs[n] = jnp.concatenate([syr[e, n : n + 1, :] for e in range(NE)], axis=0)
            part = pcodes[1, k] * at_ranks(pcodes[0, k], szs[n])
            means[0, pl.ds(z_of(k), 1), :] = jnp.sum(part, axis=0, keepdims=True)
        for k in range(1, NK):
            mean_copy(k).start()
        for k in range(1, NK):
            sz_copy(k).start()
        smat[pl.ds(pl.multiple_of(z * NE, NE), NE), :] = szs[place_of(0)]

    def dy_copy(d):
        j = (yc + d) % NE
        return remote(dys, de.at[yc], sent.at[14], got.at[5], at_e(j), x)

    @scoped
    def scores_z():
        arrived(means.at[pl.ds(1, NK - 1)], got.at[4])
        total = means[0]
        for k in range(1, NK):
            total = total + means[k]
        dys[...] = total
        for d in range(1, NE):
            dy_copy(d).start()
        de[yc] = total

    @scoped
    def home_logits():
        arrived(smat.at[pl.ds(0, NE * (NK - 1))], got.at[3])
        code_t, gate_t = codes_of(tiles[0], 0, n_exp)
        score_at = at_ranks(code_t, smat)
        mean = jnp.sum(gate_t * score_at, axis=0, keepdims=True)
        dmat[...] = jnp.where(code_t >= 0.0, gate_t * (score_at - mean), 0.0)

    x_rows = pl.ds(pl.multiple_of(x * 512, 512), 512)

    @scoped
    def token_out():
        d_t = dmat[...]
        d_hi = d_t.astype(BF16)
        d_lo = (d_t - d_hi.astype(F32)).astype(BF16)
        rw_x = rwv[:, x_rows]
        total = (dot_first(d_hi, rw_x) + dot_first(d_lo, rw_x))[0:n_tok, :]
        arrived(hxr, got.at[7])
        total = total + hxs[x].astype(F32)
        for d in range(3):
            total = total + hxr[d].astype(F32)
        arrived(wrecv.at[pl.ds(3, NK - 3)], got.at[1])
        for k in range(3, NK):
            total = total + wrecv[k].astype(F32)
        tg_ref[...] = total.astype(BF16)

    @scoped
    def router_out():
        arrived(de.at[pl.ds(0, NE - 1)], got.at[5])
        shape = (NE, CAP, 128)
        want = lax.broadcasted_iota(jnp.int32, shape, 1).astype(F32)
        lane = lax.broadcasted_iota(jnp.int32, shape, 2)
        sub = lax.broadcasted_iota(jnp.int32, shape, 1)
        sums = jnp.zeros((CAP, 512), F32)

        def of_slots(mask, rows):
            wide = jnp.where(mask, jnp.broadcast_to(rows[:, None, :], shape), 0.0)
            return jnp.sum(wide, axis=2, keepdims=True)

        for n in range(NK):
            mean = jnp.concatenate([de[j, pl.ds(z_of(block_at(n)), 1), :] for j in range(NE)], axis=0)
            code, gate = codes[0, n], codes[1, n]
            mine = jnp.broadcast_to(code[:, None, :], shape) == want
            score = of_slots(lane == sub, sx[1, n * NE : (n + 1) * NE, :])
            slot_d = of_slots(mine, gate) * (score - of_slots(mine, mean))
            rows = buf[0, n * NE : (n + 1) * NE, :, x_rows].astype(F32)
            sums = sums + jnp.sum(slot_d * rows, axis=0)
        rg_ref[...] = jnp.sum(sums, axis=0, keepdims=True)

    wide_combine(0)
    wide_combine(1)
    reduce_first(2)
    scores_x()
    weight_tiles(0, 1)
    reduce_first(3)
    reduce_second(1)
    weight_tiles(1, 2)
    reduce_second(2)
    scores_y()
    wide_combine(2)
    wide_home()
    reduce_second(3)
    combine(1)
    weight_tiles(2, 4)
    combine(2)
    combine(3)
    scores_z()
    weight_tiles(4, 8)
    home_logits()
    router_out()
    token_out()

    with jax.named_scope("drain_all"):
        seven = pl.ds(0, 7)
        for i, ref in enumerate(
            (
                zbuf.at[seven],
                tiles.at[seven],
                etiles.at[seven, pl.ds(0, 64)],
                buf.at[0, pl.ds(0, 4 * (NK - len(DIRECT)))],
                buf.at[0, pl.ds(0, 5 * NK + 2 * len(DIRECT))],
                buf.at[0],
                sx.at[pl.ds(0, 3)],
                r1.at[:, pl.ds(0, 5 * NE)],
                s2.at[pl.ds(0, 5 * NE)],
                yret.at[seven, pl.ds(0, 5)],
                wsend.at[pl.ds(0, 5)],
                sy.at[seven],
                szs.at[seven],
                means.at[seven],
                means.at[seven],
                wide.at[:, seven],
                hzr,
                hxr,
            )
        ):
            arrived(ref, sent.at[i])


def finish_kernel(tg, rg, gg, ug, dg, tg_o, rg_o, gg_o, ug_o, dg_o, sems):
    pairs = ((gg, gg_o), (ug, ug_o), (dg, dg_o), (tg, tg_o), (rg, rg_o))
    copies = [pltpu.make_async_copy(a, b, sems.at[i]) for i, (a, b) in enumerate(pairs)]
    for c in copies:
        c.start()
    for c in copies:
        c.wait()


def per_device(tokens, out_grad, expert_ids, router_weight, w_gate, w_up, w_down):
    n_tok, width = tokens.shape
    n_exp = router_weight.shape[1]
    top_count = expert_ids.shape[1]
    ff = w_gate.shape[2]
    quarter = width // 4
    any_space = pl.BlockSpec(memory_space=pl.ANY)
    vmem = pl.BlockSpec(memory_space=pltpu.VMEM)
    hbm = pl.BlockSpec(memory_space=pltpu.HBM)
    dma = pltpu.SemaphoreType.DMA
    slots = NK * NE
    scratch = [
        pltpu.VMEM((n_tok, width), BF16),
        pltpu.VMEM((top_count, n_tok), jnp.int32),
        pltpu.VMEM((n_exp, width), BF16),
        pltpu.VMEM((width, ff), BF16),
        pltpu.VMEM((width, ff), BF16),
        pltpu.VMEM((ff, width), BF16),
        pltpu.VMEM((NK, n_tok, width), BF16),
        pltpu.VMEM((NK, 8, 128), F32),
        pltpu.VMEM((NK, NE * 8, 128), F32),
        pltpu.VMEM((2, NK, NE, 128), F32),
        pltpu.VMEM((2, NK, NE, 128), F32),
        pltpu.VMEM((128, 128), BF16),
        pltpu.VMEM((NK, 2, CAP, width), BF16),
        pltpu.VMEM((NK, NE * CAP, 128), BF16),
        pltpu.VMEM((NK, NE, CAP, width), BF16),
        pltpu.VMEM((2, slots, CAP, width), BF16),
        pltpu.VMEM((slots * CAP, 2 * ff), BF16),
        pltpu.VMEM((slots * CAP, ff), BF16),
        pltpu.VMEM((4, slots, CAP, quarter), BF16),
        pltpu.VMEM((2, slots, CAP, quarter), BF16),
        pltpu.VMEM((slots, CAP, quarter), F32),
        pltpu.VMEM((slots, CAP, quarter), BF16),
        pltpu.VMEM((slots, CAP, quarter), BF16),
        pltpu.VMEM((NE, NK, CAP, quarter), BF16),
        pltpu.VMEM((NE, NK, CAP, quarter), BF16),
        pltpu.VMEM((3, NE, 4, CAP, quarter), BF16),
        pltpu.VMEM((3, 4, n_tok, quarter), BF16),
        pltpu.VMEM((2, 4, n_tok, quarter), BF16),
        pltpu.VMEM((4, n_tok, quarter), BF16),
        pltpu.VMEM((3, n_tok, quarter), BF16),
        pltpu.VMEM((NK, n_tok, quarter), BF16),
        pltpu.VMEM((NK, n_tok, quarter), BF16),
        pltpu.VMEM((4, slots, 128), F32),
        pltpu.VMEM((NE, NK, 128), F32),
        pltpu.VMEM((NE, NK, 128), F32),
        pltpu.VMEM((NK, NE, 128), F32),
        pltpu.VMEM((n_exp, 128), F32),
        pltpu.VMEM((n_exp, 128), F32),
        pltpu.VMEM((NK, NK, 128), F32),
        pltpu.VMEM((NK, 128), F32),
        pltpu.VMEM((NE, NK, 128), F32),
        dma((7,)),
        dma((18,)),
        dma((8,)),
        dma((8, 2)),
        dma((8,)),
        dma((8,)),
        dma((8,)),
        dma((8,)),
        dma((8,)),
        dma((4, 2)),
        dma((4,)),
        dma((4,)),
        dma((3,)),
    ]
    shapes = (
        jax.ShapeDtypeStruct((n_tok, quarter), BF16),
        jax.ShapeDtypeStruct((1, quarter), F32),
        jax.ShapeDtypeStruct((width, ff), BF16),
        jax.ShapeDtypeStruct((width, ff), BF16),
        jax.ShapeDtypeStruct((ff, width), BF16),
    )
    out = pl.pallas_call(
        step_kernel,
        name="moe_backward",
        out_shape=shapes,
        in_specs=[hbm] * 7,
        out_specs=(vmem,) * 5,
        scratch_shapes=scratch,
        compiler_params=pltpu.CompilerParams(
            collective_id=0, has_side_effects=True, vmem_limit_bytes=40 * 1024 * 1024
        ),
    )(
        *(
            pltpu.with_memory_space_constraint(a, pltpu.HBM)
            for a in (
                tokens,
                out_grad,
                expert_ids.T,
                router_weight.T,
                w_gate[0],
                w_up[0],
                w_down[0],
            )
        )
    )
    token_grad, router_grad, gate_grad, up_grad, down_grad = pl.pallas_call(
        finish_kernel,
        name="finish",
        out_shape=shapes,
        in_specs=[any_space] * 5,
        out_specs=(any_space,) * 5,
        scratch_shapes=[dma((5,))],
        compiler_params=pltpu.CompilerParams(vmem_limit_bytes=4 * 1024 * 1024),
    )(*out)
    return (
        token_grad,
        router_grad.reshape(quarter, 1),
        gate_grad[None],
        up_grad[None],
        down_grad[None],
    )


def solution(mesh):
    in_specs = (
        P("ep", None),
        P("ep", None),
        P("ep", None),
        P(),
        P("ep", None, "tp"),
        P("ep", None, "tp"),
        P("ep", "tp", None),
    )
    out_specs = (
        P("ep", "tp"),
        P("tp", "ep"),
        P("ep", None, "tp"),
        P("ep", None, "tp"),
        P("ep", "tp", None),
    )
    return jax.shard_map(
        per_device, mesh=mesh, in_specs=in_specs, out_specs=out_specs, check_vma=False
    )
```

```python
import functools

import jax
import jax.numpy as jnp
from jax import lax
from jax.experimental import pallas as pl
from jax.experimental.pallas import tpu as pltpu
from jax.sharding import PartitionSpec as P

MESH = pl.DeviceIdType.MESH
F32 = jnp.float32
BF16 = jnp.bfloat16
NK = 8
NE = 8
CAP = 8
PAIR_OF = (0, 2, 1, 4, 3, 6, 5, 7)
GROUPS = ((0, 2), (2, 2), (4, 2), (6, 2))
SUMMED = (None, (2, 2), (4, 2), (6, 1))
WIDE = (1, 2, 0)
DIRECT = (1, 2)


def place_of(k):
    return (k + NK - 1) % NK


def block_at(n):
    return (n + 1) % NK


def scoped(f):
    @functools.wraps(f)
    def run(*args):
        with jax.named_scope(f.__name__):
            return f(*args)

    return run


def dot_last(a, b):
    return lax.dot_general(a, b, (((1,), (1,)), ((), ())), preferred_element_type=F32)


def dot_first(a, b):
    return lax.dot_general(a, b, (((0,), (0,)), ((), ())), preferred_element_type=F32)


def dot(a, b):
    return jnp.dot(a, b, preferred_element_type=F32)


def step_kernel(
    tok_hbm,
    grad_hbm,
    ids_hbm,
    rw_hbm,
    wg_hbm,
    wu_hbm,
    wd_hbm,
    tg_ref,
    rg_ref,
    gg_ref,
    ug_ref,
    dg_ref,
    tokv,
    idsv,
    rwv,
    wg,
    wu,
    wd,
    wgt,
    wut,
    wdt,
    zbuf,
    tiles,
    etiles,
    codes,
    pcodes,
    upper,
    transit,
    pbuf,
    ysend,
    buf,
    dgu,
    wtd,
    dxq,
    r1,
    acc,
    s2,
    r2,
    yret,
    yrr,
    wide,
    hzs,
    hzr,
    hxs,
    hxr,
    wsend,
    wrecv,
    sx,
    sy,
    syr,
    szs,
    smat,
    dmat,
    means,
    dys,
    de,
    ld,
    sent,
    got,
    zrs,
    irs,
    ers,
    trs,
    yrs,
    xrs,
    r1r,
    r2r,
    vrs,
    wyr,
):
    ep = lax.axis_index("ep")
    x = lax.axis_index("tp")
    z = ep // NE
    yc = ep % NE
    y = yc // 2
    core = yc % 2
    par = x % 2
    odd = x % 2
    near_a = x + 1 - 2 * odd
    near_b = (x + 3 + 2 * odd) % 4
    far = (x + 2) % 4
    right = (x + 1) % 4
    left = (x + 3) % 4

    def remote(src, dst, ss, rs, e, t):
        return pltpu.make_async_remote_copy(
            src_ref=src,
            dst_ref=dst,
            send_sem=ss,
            recv_sem=rs,
            device_id={"ep": e, "tp": t},
            device_id_type=MESH,
        )

    def arrived(ref, sem):
        pltpu.make_async_copy(ref, ref, sem).wait()

    def z_of(k):
        h = (k + 1) // 2
        s = 1 - 2 * ((k + 1) % 2)
        return (z + s * h + NK) % NK

    def at_z(zz):
        return zz * NE + yc

    def at_e(j):
        return z * NE + j

    def in_plane(dy, c):
        return ((y + dy + 4) % 4) * 2 + c

    barrier = pltpu.get_barrier_semaphore()
    for d in (1, NK - 1):
        pl.semaphore_signal(
            barrier, inc=1, device_id={"ep": at_z((z + d) % NK), "tp": x}, device_id_type=MESH
        )
    for d in range(1, NE):
        pl.semaphore_signal(
            barrier, inc=1, device_id={"ep": at_e((yc + d) % NE), "tp": x}, device_id_type=MESH
        )
    for d in range(1, 4):
        pl.semaphore_signal(
            barrier, inc=1, device_id={"ep": ep, "tp": (x + d) % 4}, device_id_type=MESH
        )

    load_tok = pltpu.make_async_copy(tok_hbm, tokv, ld.at[0])
    load_tok.start()
    load_ids = pltpu.make_async_copy(ids_hbm, idsv, ld.at[5])
    load_rw = pltpu.make_async_copy(rw_hbm, rwv, ld.at[6])
    load_ids.start()
    load_rw.start()

    @pl.when(par == 0)
    def _():
        pltpu.make_async_copy(tok_hbm, zbuf.at[0], ld.at[1]).start()

    @pl.when(par == 1)
    def _():
        pltpu.make_async_copy(grad_hbm, zbuf.at[0], ld.at[1]).start()

    load_g = pltpu.make_async_copy(wg_hbm, wg, ld.at[2])
    load_u = pltpu.make_async_copy(wu_hbm, wu, ld.at[3])
    load_d = pltpu.make_async_copy(wd_hbm, wd, ld.at[4])
    load_g.start()
    load_u.start()
    load_d.start()

    @scoped
    def wait_small():
        load_tok.wait()
        load_ids.wait()
        load_rw.wait()

    @scoped
    def wait_barrier():
        pl.semaphore_wait(barrier, 2 + (NE - 1) + 3)

    wait_barrier()

    pltpu.make_async_copy(tok_hbm, zbuf.at[0], ld.at[1]).wait()

    half = zbuf.shape[2] // 2

    def z_copy(k, part):
        to = 7 if k >= 5 else k + 2
        s = 1 - 2 * ((k + 1) % 2)
        cols = pl.ds(part * half, half)
        return remote(
            zbuf.at[k, :, cols],
            zbuf.at[to, :, cols],
            sent.at[0],
            zrs.at[to, part],
            at_z((z - s + NK) % NK),
            x,
        )

    def z_first(part, way):
        cols = pl.ds(part * half, half)
        return remote(
            zbuf.at[0, :, cols],
            zbuf.at[1 + way, :, cols],
            sent.at[0],
            zrs.at[1 + way, part],
            at_z((z + 1) % NK) if way else at_z((z + NK - 1) % NK),
            x,
        )

    def tile_copy(k):
        s = 1 - 2 * ((k + 1) % 2)
        return remote(
            tiles.at[k], tiles.at[k + 2], sent.at[1], irs.at[k + 2], at_z((z - s + NK) % NK), x
        )

    below, above = at_z((z + NK - 1) % NK), at_z((z + 1) % NK)
    t_left = remote(tiles.at[0], tiles.at[1], sent.at[1], irs.at[1], below, x)
    t_right = remote(tiles.at[0], tiles.at[2], sent.at[1], irs.at[2], above, x)
    z_first(0, 0).start()
    z_first(0, 1).start()
    wait_small()
    n_tok = tokv.shape[0]
    n_exp = rwv.shape[0]
    logits = dot_last(rwv[...], tokv[...])
    expert = lax.broadcasted_iota(jnp.int32, (n_exp, n_tok), 0)
    picked = []
    for k in range(idsv.shape[0]):
        here = idsv[k : k + 1, :] == expert
        picked.append(jnp.sum(jnp.where(here, logits, 0.0), axis=0, keepdims=True))
    picked = jnp.concatenate(picked, axis=0)
    expd = jnp.exp(picked - jnp.max(picked, axis=0, keepdims=True))
    gates = expd / jnp.sum(expd, axis=0, keepdims=True)
    tiles[0] = jnp.full((8, 128), -1.0, F32)
    tiles[0, 0:4, 0:n_tok] = idsv[...].astype(F32)
    tiles[0, 4:8, 0:n_tok] = gates
    row = lax.broadcasted_iota(jnp.int32, (128, 128), 0)
    col = lax.broadcasted_iota(jnp.int32, (128, 128), 1)
    upper[...] = jnp.where(row < col, 1.0, 0.0).astype(BF16)

    def rank_of(hit):
        return jnp.where(hit > 0.0, dot(hit.astype(BF16), upper[...]), -1.0)

    def codes_of(tile, first, count):
        experts = (lax.broadcasted_iota(jnp.int32, (count, 128), 0) + first).astype(F32)
        hit = jnp.zeros((count, 128), F32)
        gate = jnp.zeros((count, 128), F32)
        for k in range(4):
            here = tile[k : k + 1, :] == experts
            hit = hit + jnp.where(here, 1.0, 0.0)
            gate = gate + jnp.where(here, tile[4 + k : 5 + k, :], 0.0)
        return rank_of(hit), gate

    t_left.start()
    t_right.start()
    z_first(1, 0).start()
    z_first(1, 1).start()

    def share_copy(k, d):
        j = (yc + d) % NE
        return remote(
            tiles.at[k],
            etiles.at[k, pl.ds(pl.multiple_of(yc * 8, 8), 8)],
            sent.at[2],
            ers.at[k],
            at_e(j),
            x,
        )

    def share_wait(k):
        arrived(etiles.at[k, pl.ds(0, 8 * (NE - 1))], ers.at[k])

    steps = ((1, 0), (1, 1), (-1, 0), (-1, 1))

    def transit_copy(k, way, cols):
        e = in_plane(2, way)
        return remote(
            ysend.at[k, e],
            transit.at[k, way],
            sent.at[3],
            trs.at[k],
            at_e(in_plane(-1 if way else 1, core)),
            x,
        )

    def direct_copy(k, way, cols):
        e = in_plane(2, way)
        return remote(
            ysend.at[k, e, :, cols],
            buf.at[par, place_of(k) * NE + yc, :, cols],
            sent.at[4],
            yrs.at[k],
            at_e(e),
            x,
        )

    def near_copy(k, n, cols):
        j = in_plane(*steps[n]) if n < 4 else in_plane(0, 1 - core)
        return remote(
            ysend.at[k, j, :, cols],
            buf.at[par, place_of(k) * NE + yc, :, cols],
            sent.at[4],
            yrs.at[k],
            at_e(j),
            x,
        )

    def forward_copy(k, way):
        src = in_plane(1 if way else -1, core)
        return remote(
            transit.at[k, way],
            buf.at[par, place_of(k) * NE + src],
            sent.at[3],
            yrs.at[k],
            at_e(in_plane(-1 if way else 1, way)),
            x,
        )

    @scoped
    def take(k, part):
        if part == 0:
            arrived(tiles.at[k], irs.at[k])
            if k <= 5:
                tile_copy(k).start()
        cols = pl.ds(part * half, half)
        arrived(zbuf.at[k, :, cols], zrs.at[k, part])
        if k <= 4 or (k, part) in ((5, 1), (6, 0)):
            z_copy(k, part).start()

    @scoped
    def select_block(k):
        place_block(k)
        send_rows(k, slice(0, 2 * half))

    def place_block(k):
        for d in range(1, NE):
            share_copy(k, d).start()
        tile = tiles[k]
        etiles[k, pl.ds(pl.multiple_of(yc * 8, 8), 8)] = tile
        code, gate = codes_of(tile, z * NE, NE)
        pcodes[0, k] = code
        pcodes[1, k] = gate
        want = lax.broadcasted_iota(jnp.int32, (NE, CAP, 128), 1).astype(F32)
        place = (jnp.broadcast_to(code[:, None, :], (NE, CAP, 128)) == want).astype(F32)
        pbuf[k] = place.reshape(NE * CAP, 128).astype(BF16)

    def send_rows(k, cols):
        place = pbuf[k]
        for q in range(cols.start, cols.stop, 512):
            rows = dot(place[:, 0:n_tok], zbuf[k, :, q : q + 512])
            ysend[k, :, :, q : q + 512] = rows.astype(BF16).reshape(NE, CAP, 512)
        for way in range(2):
            (direct_copy if k in DIRECT else transit_copy)(k, way, cols).start()
        for n in (0, 2, 1, 3, 4):
            near_copy(k, n, cols).start()
        buf[par, place_of(k) * NE + yc, :, cols] = ysend[k, yc, :, cols]

    @scoped
    def hand_over(k):
        arrived(transit.at[k], trs.at[k])
        for way in range(2):
            forward_copy(k, way).start()

    half_e = NE // 2

    def x_copy(k, side):
        rows = pl.ds(place_of(k) * NE + side * half_e, half_e)
        return remote(
            buf.at[par, rows],
            buf.at[par, rows],
            sent.at[5],
            xrs.at[k],
            ep,
            left if side else right,
        )

    @scoped
    def x_waits(k):
        arrived(buf.at[1 - par, pl.ds(place_of(k) * NE, NE)], xrs.at[k])

    @scoped
    def y_waits(k):
        arrived(buf.at[par, pl.ds(place_of(k) * NE, NE - 1)], yrs.at[k])

    @scoped
    def pass_on(k):
        y_waits(k)
        x_copy(k, 0).start()
        x_copy(k, 1).start()

    def slot_info(k):
        hit = jnp.zeros((NE, 128), F32)
        gate = jnp.zeros((NE, 128), F32)
        mine = ep.astype(F32)
        for c in range(4):
            here = etiles[k, pl.ds(c, NE, stride=8), :] == mine
            hit = hit + jnp.where(here, 1.0, 0.0)
            gate = gate + jnp.where(here, etiles[k, pl.ds(4 + c, NE, stride=8), :], 0.0)
        return rank_of(hit), gate

    def score_copy(m, d):
        t = (x + d) % 4
        rows = pl.ds(GROUPS[m][0] * NE, GROUPS[m][1] * NE)
        return remote(sx.at[0, rows], sx.at[4 - d, rows], sent.at[6], got.at[0], ep, t)

    def unit(m, which):
        n, count = SUMMED[m]
        return pl.ds(n * NE + which * count * NE // 2, count * NE // 2)

    def halves_copy(m, which, slot):
        peer = near_b if which else near_a
        q = far if slot else peer
        rows = unit(m, which)
        return remote(
            dxq.at[q, rows], r1.at[slot, rows], sent.at[7], r1r.at[m, slot], ep, peer
        )

    def group(m):
        n, count = SUMMED[m]
        return pl.ds(n * NE, count * NE)

    @scoped
    def turn_down():
        load_d.wait()
        for i in range(0, 2048, 256):
            wdt[i : i + 256, :] = wd[:, i : i + 256].T

    @scoped
    def turn(load, w, wt):
        load.wait()
        for i in range(0, 2048, 256):
            wt[:, i : i + 256] = w[i : i + 256, :].T

    @scoped
    def compute(m):
        first, count = GROUPS[m]
        n_rows = count * NE * CAP
        infos = []
        for n in range(first, first + count):
            share_wait(block_at(n))
            infos.append(slot_info(block_at(n)))
            codes[0, n], codes[1, n] = infos[-1]
        code = jnp.concatenate([i[0] for i in infos], axis=0)
        gate = jnp.concatenate([i[1] for i in infos], axis=0)
        shape = (count * NE, CAP, 128)
        want = lax.broadcasted_iota(jnp.int32, shape, 1).astype(F32)
        mine = jnp.broadcast_to(code[:, None, :], shape) == want
        wide = jnp.where(mine, jnp.broadcast_to(gate[:, None, :], shape), 0.0)
        weight = jnp.sum(wide.reshape(n_rows, 128), axis=1, keepdims=True)
        for n in range(first, first + count):
            x_waits(block_at(n))
        rows = pl.ds(first * NE, count * NE)
        flat = pl.ds(first * NE * CAP, n_rows)
        xin = buf[0, rows].reshape(n_rows, 2048)
        gin = buf[1, rows].reshape(n_rows, 2048)
        gate_pre = dot(xin, wg[...])
        up_pre = dot(xin, wu[...])
        back = dot(gin, wdt[...])
        glu = jnp.minimum(gate_pre, 7.0)
        lin1 = jnp.clip(up_pre, -7.0, 7.0) + 1.0
        sig = jax.nn.sigmoid(1.702 * glu)
        act = glu * sig
        hidden = lin1 * act
        slope = lin1 * (sig + 1.702 * glu * sig * (1.0 - sig))
        slope = jnp.where(gate_pre < 7.0, slope, 0.0)
        up_slope = jnp.where((up_pre > -7.0) & (up_pre < 7.0), act, 0.0)
        score = jnp.sum(hidden * back, axis=1, keepdims=True)
        d_hidden = weight * back
        d_gate = (d_hidden * slope).astype(BF16)
        d_up = (d_hidden * up_slope).astype(BF16)
        dgu[flat, 0:384] = d_gate
        dgu[flat, 384:768] = d_up
        wtd[flat, :] = (weight * hidden).astype(BF16)
        lane = lax.broadcasted_iota(jnp.int32, shape, 2)
        sub = lax.broadcasted_iota(jnp.int32, shape, 1)
        spread = jnp.broadcast_to(score, (n_rows, 128)).reshape(shape)
        sx[0, rows] = jnp.sum(jnp.where(lane == sub, spread, 0.0), axis=1)
        for d in range(1, 4):
            score_copy(m, d).start()

        for q in range(4):
            cols = slice(512 * q, 512 * (q + 1))
            part = dot(d_gate, wgt[:, cols]) + dot(d_up, wut[:, cols])
            dxq[q, rows] = part.astype(BF16).reshape(count * NE, CAP, 512)
    @scoped
    def send_halves(m):
        for slot in (1, 0):
            for which in range(2):
                halves_copy(m, which, slot).start()

    def quarter_copy(m, which):
        rows = unit(m, which)
        return remote(
            s2.at[rows], r2.at[rows], sent.at[8], r2r.at[m], ep, near_a if which else near_b
        )

    @scoped
    def wait_half(m, slot):
        arrived(r1.at[slot, group(m)], r1r.at[m, slot])

    @scoped
    def wait_quarter(m):
        arrived(r2.at[group(m)], r2r.at[m])

    @scoped
    def reduce_first(m):
        wait_half(m, 1)
        for which in range(2):
            rows = unit(m, which)
            s2[rows] = (
                dxq[near_a if which else near_b, rows].astype(F32) + r1[1, rows].astype(F32)
            ).astype(BF16)
            quarter_copy(m, which).start()
        wait_half(m, 0)
        for which in range(2):
            rows = unit(m, which)
            acc[rows] = dxq[x, rows].astype(F32) + r1[0, rows].astype(F32)

    def back_copy(m, d):
        j = (yc + d) % NE
        ks = pl.ds(*SUMMED[m])
        return remote(yret.at[j, ks], yrr.at[yc, ks], sent.at[9], vrs.at[m], at_e(j), x)

    @scoped
    def reduce_second(m):
        first, count = SUMMED[m]
        wait_quarter(m)
        for k in range(first, first + count):
            rows = pl.ds(k * NE, NE)
            total = (acc[rows] + r2[rows].astype(F32)).astype(BF16)
            for j in range(NE):
                yret[j, k] = total[j]
        for d in (1, 7, 2, 6, 3, 5, 4):
            back_copy(m, d).start()
        ks = pl.ds(first, count)
        yrr[yc, ks] = yret[yc, ks]

    def home_copy(k):
        return remote(
            wsend.at[k], wrecv.at[PAIR_OF[k]], sent.at[10], got.at[1], at_z(z_of(k)), x
        )

    @scoped
    def back_waits(m):
        arrived(yrr.at[pl.ds(0, NE - 1), pl.ds(*SUMMED[m])], vrs.at[m])

    @scoped
    def combine(m):
        back_waits(m)
        first, count = SUMMED[m]
        for n in range(first, first + count):
            k = block_at(n)
            rows = jnp.concatenate([yrr[j, n] for j in range(NE)], axis=0)
            wsend[k] = dot_first(pbuf[k][:, 0:n_tok], rows).astype(BF16)
            home_copy(k).start()

    @scoped
    def wide_send(w):
        n = place_of(WIDE[w])
        for d in (1, 7, 2, 6, 3, 5, 4):
            j = (yc + d) % NE
            remote(
                dxq.at[:, n * NE + j], wide.at[w, yc], sent.at[15], wyr.at[w], at_e(j), x
            ).start()
        wide[w, yc] = dxq[:, n * NE + yc]

    @scoped
    def wide_combine(w):
        arrived(wide.at[w, pl.ds(0, NE - 1)], wyr.at[w])
        k = WIDE[w]
        place = pbuf[k][:, 0:n_tok]
        for q in range(4):
            rows = jnp.concatenate([wide[w, j, q] for j in range(NE)], axis=0)
            hzs[w, q] = dot_first(place, rows).astype(BF16)
        if k:
            remote(
                hzs.at[w], hzr.at[PAIR_OF[k] - 1], sent.at[16], got.at[6], at_z(z_of(k)), x
            ).start()

    @scoped
    def wide_home():
        arrived(hzr, got.at[6])
        hxs[...] = (
            hzs[2].astype(F32) + hzr[0].astype(F32) + hzr[1].astype(F32)
        ).astype(BF16)
        for d in (1, 3, 2):
            t = (x + d) % 4
            remote(hxs.at[t], hxr.at[3 - d], sent.at[17], got.at[7], ep, t).start()

    def both(f, *ks):
        for k in ks:
            f(k)

    def takes(part, *ks):
        for k in ks:
            take(k, part)

    first_half, second_half = slice(0, half), slice(half, 2 * half)
    select_block(0)
    hand_over(0)
    takes(0, 1, 2)
    place_block(1)
    send_rows(1, first_half)
    place_block(2)
    send_rows(2, first_half)
    takes(1, 1, 2)
    send_rows(1, second_half)
    send_rows(2, second_half)
    takes(0, 3, 4)
    pass_on(0)
    takes(1, 3, 4)
    select_block(3)
    turn_down()
    pass_on(1)
    select_block(4)
    pass_on(2)
    hand_over(3)
    takes(0, 5, 6)
    hand_over(4)
    takes(1, 5, 6)
    select_block(5)
    turn(load_g, wg, wgt)
    pass_on(3)
    select_block(6)
    take(7, 0)
    take(7, 1)
    hand_over(5)
    select_block(7)
    pass_on(4)
    turn(load_u, wu, wut)
    hand_over(6)
    compute(0)
    pass_on(5)
    hand_over(7)
    wide_send(0)
    wide_send(1)
    pass_on(6)
    pass_on(7)
    compute(1)
    send_halves(1)
    compute(2)
    send_halves(2)
    compute(3)
    send_halves(3)
    wide_send(2)
    reduce_first(1)

    @scoped
    def weight_tile(i, carry):
        cols = pl.ds(pl.multiple_of(i * 256, 256), 256)
        xs = buf[0, :, :, cols].reshape(512, 256)
        both = dot_first(xs, dgu[...]).astype(BF16)
        gg_ref[cols, :] = both[:, 0:384]
        ug_ref[cols, :] = both[:, 384:768]
        gs = buf[1, :, :, cols].reshape(512, 256)
        dg_ref[:, cols] = dot_first(wtd[...], gs).astype(BF16)
        return carry

    def weight_tiles(a, b):
        lax.fori_loop(a, b, weight_tile, 0)

    def sy_copy(d):
        j = (yc + d) % NE
        return remote(sy.at[j], syr.at[yc], sent.at[11], got.at[2], at_e(j), x)

    @scoped
    def scores_x():
        arrived(sx.at[pl.ds(1, 3)], got.at[0])
        sx[1] = (sx[0] + sx[1]) + (sx[2] + sx[3])
        for j in range(NE):
            sy[j] = jnp.concatenate(
                [sx[1, k * NE + j : k * NE + j + 1, :] for k in range(NK)], axis=0
            )
        for d in range(1, NE):
            sy_copy(d).start()
        syr[yc] = sy[yc]

    def sz_copy(k):
        return remote(
            szs.at[place_of(k)],
            smat.at[pl.ds(pl.multiple_of(z * NE, NE), NE)],
            sent.at[12],
            got.at[3],
            at_z(z_of(k)),
            x,
        )

    def mean_copy(k):
        return remote(
            means.at[0],
            means.at[PAIR_OF[k]],
            sent.at[13],
            got.at[4],
            at_z(z_of(k)),
            x,
        )

    def at_ranks(code, scores):
        found = jnp.zeros(code.shape, F32)
        for r in range(CAP):
            found = found + jnp.where(code == float(r), scores[:, r : r + 1], 0.0)
        return found

    @scoped
    def scores_y():
        arrived(syr.at[pl.ds(0, NE - 1)], got.at[2])
        for n in range(NK):
            k = block_at(n)
            szs[n] = jnp.concatenate([syr[e, n : n + 1, :] for e in range(NE)], axis=0)
            part = pcodes[1, k] * at_ranks(pcodes[0, k], szs[n])
            means[0, pl.ds(z_of(k), 1), :] = jnp.sum(part, axis=0, keepdims=True)
        for k in range(1, NK):
            mean_copy(k).start()
        for k in range(1, NK):
            sz_copy(k).start()
        smat[pl.ds(pl.multiple_of(z * NE, NE), NE), :] = szs[place_of(0)]

    def dy_copy(d):
        j = (yc + d) % NE
        return remote(dys, de.at[yc], sent.at[14], got.at[5], at_e(j), x)

    @scoped
    def scores_z():
        arrived(means.at[pl.ds(1, NK - 1)], got.at[4])
        total = means[0]
        for k in range(1, NK):
            total = total + means[k]
        dys[...] = total
        for d in range(1, NE):
            dy_copy(d).start()
        de[yc] = total

    @scoped
    def home_logits():
        arrived(smat.at[pl.ds(0, NE * (NK - 1))], got.at[3])
        code_t, gate_t = codes_of(tiles[0], 0, n_exp)
        score_at = at_ranks(code_t, smat)
        mean = jnp.sum(gate_t * score_at, axis=0, keepdims=True)
        dmat[...] = jnp.where(code_t >= 0.0, gate_t * (score_at - mean), 0.0)

    x_rows = pl.ds(pl.multiple_of(x * 512, 512), 512)

    @scoped
    def token_out():
        d_t = dmat[...]
        d_hi = d_t.astype(BF16)
        d_lo = (d_t - d_hi.astype(F32)).astype(BF16)
        rw_x = rwv[:, x_rows]
        total = (dot_first(d_hi, rw_x) + dot_first(d_lo, rw_x))[0:n_tok, :]
        arrived(hxr, got.at[7])
        total = total + hxs[x].astype(F32)
        for d in range(3):
            total = total + hxr[d].astype(F32)
        arrived(wrecv.at[pl.ds(3, NK - 3)], got.at[1])
        for k in range(3, NK):
            total = total + wrecv[k].astype(F32)
        tg_ref[...] = total.astype(BF16)

    @scoped
    def router_out():
        arrived(de.at[pl.ds(0, NE - 1)], got.at[5])
        shape = (NE, CAP, 128)
        want = lax.broadcasted_iota(jnp.int32, shape, 1).astype(F32)
        lane = lax.broadcasted_iota(jnp.int32, shape, 2)
        sub = lax.broadcasted_iota(jnp.int32, shape, 1)
        sums = jnp.zeros((CAP, 512), F32)

        def of_slots(mask, rows):
            wide = jnp.where(mask, jnp.broadcast_to(rows[:, None, :], shape), 0.0)
            return jnp.sum(wide, axis=2, keepdims=True)

        for n in range(NK):
            mean = jnp.concatenate([de[j, pl.ds(z_of(block_at(n)), 1), :] for j in range(NE)], axis=0)
            code, gate = codes[0, n], codes[1, n]
            mine = jnp.broadcast_to(code[:, None, :], shape) == want
            score = of_slots(lane == sub, sx[1, n * NE : (n + 1) * NE, :])
            slot_d = of_slots(mine, gate) * (score - of_slots(mine, mean))
            rows = buf[0, n * NE : (n + 1) * NE, :, x_rows].astype(F32)
            sums = sums + jnp.sum(slot_d * rows, axis=0)
        rg_ref[...] = jnp.sum(sums, axis=0, keepdims=True)

    wide_combine(0)
    wide_combine(1)
    reduce_first(2)
    scores_x()
    weight_tiles(0, 1)
    reduce_first(3)
    reduce_second(1)
    weight_tiles(1, 2)
    reduce_second(2)
    scores_y()
    wide_combine(2)
    wide_home()
    reduce_second(3)
    combine(1)
    weight_tiles(2, 4)
    combine(2)
    combine(3)
    scores_z()
    weight_tiles(4, 8)
    home_logits()
    router_out()
    token_out()

    with jax.named_scope("drain_all"):
        seven = pl.ds(0, 7)
        for i, ref in enumerate(
            (
                zbuf.at[seven],
                tiles.at[seven],
                etiles.at[seven, pl.ds(0, 64)],
                buf.at[0, pl.ds(0, 4 * (NK - len(DIRECT)))],
                buf.at[0, pl.ds(0, 5 * NK + 2 * len(DIRECT))],
                buf.at[0],
                sx.at[pl.ds(0, 3)],
                r1.at[:, pl.ds(0, 5 * NE)],
                s2.at[pl.ds(0, 5 * NE)],
                yret.at[seven, pl.ds(0, 5)],
                wsend.at[pl.ds(0, 5)],
                sy.at[seven],
                szs.at[seven],
                means.at[seven],
                means.at[seven],
                wide.at[:, seven],
                hzr,
                hxr,
            )
        ):
            arrived(ref, sent.at[i])


def finish_kernel(tg, rg, gg, ug, dg, tg_o, rg_o, gg_o, ug_o, dg_o, sems):
    pairs = ((gg, gg_o), (ug, ug_o), (dg, dg_o), (tg, tg_o), (rg, rg_o))
    copies = [pltpu.make_async_copy(a, b, sems.at[i]) for i, (a, b) in enumerate(pairs)]
    for c in copies:
        c.start()
    for c in copies:
        c.wait()


def per_device(tokens, out_grad, expert_ids, router_weight, w_gate, w_up, w_down):
    n_tok, width = tokens.shape
    n_exp = router_weight.shape[1]
    top_count = expert_ids.shape[1]
    ff = w_gate.shape[2]
    quarter = width // 4
    any_space = pl.BlockSpec(memory_space=pl.ANY)
    vmem = pl.BlockSpec(memory_space=pltpu.VMEM)
    hbm = pl.BlockSpec(memory_space=pltpu.HBM)
    dma = pltpu.SemaphoreType.DMA
    slots = NK * NE
    scratch = [
        pltpu.VMEM((n_tok, width), BF16),
        pltpu.VMEM((top_count, n_tok), jnp.int32),
        pltpu.VMEM((n_exp, width), BF16),
        pltpu.VMEM((width, ff), BF16),
        pltpu.VMEM((width, ff), BF16),
        pltpu.VMEM((ff, width), BF16),
        pltpu.VMEM((ff, width), BF16),
        pltpu.VMEM((ff, width), BF16),
        pltpu.VMEM((width, ff), BF16),
        pltpu.VMEM((NK, n_tok, width), BF16),
        pltpu.VMEM((NK, 8, 128), F32),
        pltpu.VMEM((NK, NE * 8, 128), F32),
        pltpu.VMEM((2, NK, NE, 128), F32),
        pltpu.VMEM((2, NK, NE, 128), F32),
        pltpu.VMEM((128, 128), BF16),
        pltpu.VMEM((NK, 2, CAP, width), BF16),
        pltpu.VMEM((NK, NE * CAP, 128), BF16),
        pltpu.VMEM((NK, NE, CAP, width), BF16),
        pltpu.VMEM((2, slots, CAP, width), BF16),
        pltpu.VMEM((slots * CAP, 2 * ff), BF16),
        pltpu.VMEM((slots * CAP, ff), BF16),
        pltpu.VMEM((4, slots, CAP, quarter), BF16),
        pltpu.VMEM((2, slots, CAP, quarter), BF16),
        pltpu.VMEM((slots, CAP, quarter), F32),
        pltpu.VMEM((slots, CAP, quarter), BF16),
        pltpu.VMEM((slots, CAP, quarter), BF16),
        pltpu.VMEM((NE, NK, CAP, quarter), BF16),
        pltpu.VMEM((NE, NK, CAP, quarter), BF16),
        pltpu.VMEM((3, NE, 4, CAP, quarter), BF16),
        pltpu.VMEM((3, 4, n_tok, quarter), BF16),
        pltpu.VMEM((2, 4, n_tok, quarter), BF16),
        pltpu.VMEM((4, n_tok, quarter), BF16),
        pltpu.VMEM((3, n_tok, quarter), BF16),
        pltpu.VMEM((NK, n_tok, quarter), BF16),
        pltpu.VMEM((NK, n_tok, quarter), BF16),
        pltpu.VMEM((4, slots, 128), F32),
        pltpu.VMEM((NE, NK, 128), F32),
        pltpu.VMEM((NE, NK, 128), F32),
        pltpu.VMEM((NK, NE, 128), F32),
        pltpu.VMEM((n_exp, 128), F32),
        pltpu.VMEM((n_exp, 128), F32),
        pltpu.VMEM((NK, NK, 128), F32),
        pltpu.VMEM((NK, 128), F32),
        pltpu.VMEM((NE, NK, 128), F32),
        dma((7,)),
        dma((18,)),
        dma((8,)),
        dma((8, 2)),
        dma((8,)),
        dma((8,)),
        dma((8,)),
        dma((8,)),
        dma((8,)),
        dma((4, 2)),
        dma((4,)),
        dma((4,)),
        dma((3,)),
    ]
    shapes = (
        jax.ShapeDtypeStruct((n_tok, quarter), BF16),
        jax.ShapeDtypeStruct((1, quarter), F32),
        jax.ShapeDtypeStruct((width, ff), BF16),
        jax.ShapeDtypeStruct((width, ff), BF16),
        jax.ShapeDtypeStruct((ff, width), BF16),
    )
    out = pl.pallas_call(
        step_kernel,
        name="moe_backward",
        out_shape=shapes,
        in_specs=[hbm] * 7,
        out_specs=(vmem,) * 5,
        scratch_shapes=scratch,
        compiler_params=pltpu.CompilerParams(
            collective_id=0, has_side_effects=True, vmem_limit_bytes=40 * 1024 * 1024
        ),
    )(
        *(
            pltpu.with_memory_space_constraint(a, pltpu.HBM)
            for a in (
                tokens,
                out_grad,
                expert_ids.T,
                router_weight.T,
                w_gate[0],
                w_up[0],
                w_down[0],
            )
        )
    )
    token_grad, router_grad, gate_grad, up_grad, down_grad = pl.pallas_call(
        finish_kernel,
        name="finish",
        out_shape=shapes,
        in_specs=[any_space] * 5,
        out_specs=(any_space,) * 5,
        scratch_shapes=[dma((5,))],
        compiler_params=pltpu.CompilerParams(vmem_limit_bytes=4 * 1024 * 1024),
    )(*out)
    return (
        token_grad,
        router_grad.reshape(quarter, 1),
        gate_grad[None],
        up_grad[None],
        down_grad[None],
    )


def solution(mesh):
    in_specs = (
        P("ep", None),
        P("ep", None),
        P("ep", None),
        P(),
        P("ep", None, "tp"),
        P("ep", None, "tp"),
        P("ep", "tp", None),
    )
    out_specs = (
        P("ep", "tp"),
        P("tp", "ep"),
        P("ep", None, "tp"),
        P("ep", None, "tp"),
        P("ep", "tp", None),
    )
    return jax.shard_map(
        per_device, mesh=mesh, in_specs=in_specs, out_specs=out_specs, check_vma=False
    )
```
